32 devices in a mesh: ep: 16 (over z, y, core), tp: 2 (over x).
Axes of the slice: x: 2, y: 2, z: 4, core: 2. Of those that a mesh axis runs over, the one named last changes fastest.
Arguments:
- tokens: bfloat16 [2048, 2048], P('ep'), may hold values from -6 to 6
- expert_ids: int32 [2048, 2], P('ep'), may hold values from 0 to 15, as said below
- route_weights: bfloat16 [2048, 2], P('ep'), may hold values from 0.099609375 to 1
- cotangent: bfloat16 [2048, 2048], P('ep'), may hold values from -3 to 3
- w_gate: bfloat16 [16, 2048, 512], P('ep', None, 'tp'), may hold values from -0.125 to 0.125
- w_up: bfloat16 [16, 2048, 512], P('ep', None, 'tp'), may hold values from -0.125 to 0.125
- w_down: bfloat16 [16, 512, 2048], P('ep', 'tp'), may hold values from -0.25 to 0.25
Outputs:
- token_grad: bfloat16 [2048, 2048], P('ep', 'tp')
- route_grad: bfloat16 [2048, 2], P('ep')
- grad_gate: bfloat16 [16, 2048, 512], P('ep', None, 'tp')
- grad_up: bfloat16 [16, 2048, 512], P('ep', None, 'tp')
- grad_down: bfloat16 [16, 512, 2048], P('ep', 'tp')
- gate_rows: float32 [16, 2048], P('ep')
- up_rows: float32 [16, 2048], P('ep')
- down_rows: float32 [16, 512], P('ep', 'tp')
The draws below stay inside these ranges and needn't reach their ends.
Inputs may be any that keep to these rules, and one draw needn't show every extreme that they name: `expert_ids`: each row names 2 different experts of one group: both lie in g * 4 to (g + 1) * 4 - 1 for the row's group g. In the rows of one device (aligned blocks of 128 rows) no expert is named more than 32 times, and in every block some expert is named exactly 32 times.
All inputs are finite; a program needn't handle non-finite values.
Results may differ from the reference program's by a relative error of at most 0.012.
Values may be sent and summed in bfloat16 or wider, within the bound.
A program may use at most 64 MiB of HBM per device.

```python
import jax
import jax.numpy as jnp
from jax import lax

D = 2048
F = 512
GROUPS = 4
TOPK = 2
TOK_DEV = 128
EXPERTS = 16
CAP = 32
TOKENS = 2048
N_EP = 16
N_TP = 2


def draw_expert_ids(key, part):
    per_group = EXPERTS // GROUPS
    blocks = TOKENS // TOK_DEV
    hot_group = jax.random.randint(jax.random.fold_in(key, 11), (), 0, GROUPS)
    hot_member = jax.random.randint(jax.random.fold_in(key, 12), (), 0, per_group)
    block_keys = jax.random.split(jax.random.fold_in(key, 13), blocks)
    group_ids = jnp.arange(GROUPS, dtype=jnp.int32)
    member_ids = jnp.arange(per_group, dtype=jnp.int32)

    def one_block(block_key):
        key_a, key_b, key_c, key_d, key_e = jax.random.split(block_key, 5)
        hot_size = jax.random.randint(key_a, (), max(CAP, TOK_DEV // 4), TOK_DEV // 2 + 1)
        remain = TOK_DEV - hot_size
        third = remain // 3
        jitter = remain // 8
        first_size = jax.random.randint(key_b, (), third - jitter, third + jitter + 1)
        second_size = jax.random.randint(key_c, (), third - jitter, third + jitter + 1)
        others = jnp.stack([first_size, second_size, remain - first_size - second_size])
        other_slot = jnp.minimum((group_ids - hot_group - 1) % GROUPS, 2)
        sizes = jnp.where(group_ids == hot_group, hot_size, others[other_slot]).astype(jnp.int32)
        ends = jnp.cumsum(sizes)
        starts = ends - sizes
        fill_step = jnp.maximum(jnp.minimum(CAP, sizes), 1)
        ranks = jax.random.permutation(key_d, TOK_DEV).astype(jnp.int32)
        member_group = jnp.sum((ranks[:, None] >= ends[None, :]).astype(jnp.int32), axis=1)
        inner = ranks - starts[member_group]
        count = sizes[member_group]
        stride = fill_step[member_group]
        scores = jax.random.randint(key_e, (GROUPS, per_group), 0, 1 << 20) * per_group + member_ids[None, :]
        pinned = (group_ids[:, None] == hot_group) & (member_ids[None, :] == hot_member)
        scores = jnp.where(pinned, -1, scores)
        ordering = jnp.argsort(scores, axis=1).astype(jnp.int32)
        first_pick = ordering[member_group, inner // stride]
        second_pick = ordering[member_group, (inner + count) // stride]
        base_ids = member_group * per_group
        return jnp.stack([base_ids + first_pick, base_ids + second_pick], axis=1)
    return jax.vmap(one_block)(block_keys).reshape(TOKENS, TOPK).astype(jnp.int32)


def block_levels(key, extent, pieces, least, largest):
    loudness = 1.0
    for position, parts in pieces:
        steps = jax.random.uniform(jax.random.fold_in(jax.random.fold_in(key, 6), position), (parts,), jnp.float32, least / len(pieces), largest / len(pieces))
        loudness = loudness * jnp.repeat(jnp.exp(steps), extent[position] // parts).reshape((-1,) + (1,) * (len(extent) - 1 - position))
    return loudness


def noise(rng, shape, spread, bound, cuts=(), kind=jnp.bfloat16):
    result = jax.random.normal(rng, shape, jnp.float32) * spread
    if len(cuts) > 0:
        result = block_levels(rng, shape, cuts, -0.22, 0.18) * result
    return jnp.clip(result, min=-bound, max=bound).astype(kind)


def setup_inputs(seed: int = 0) -> dict:
    streams_of = jax.random.split(jax.random.key(seed), 8)
    tokens = noise(streams_of[0], (TOKENS, D), 1.0, 6.0, ((0, 16),))
    expert_ids = draw_expert_ids(jax.random.fold_in(streams_of[7], 71), 0)
    route_weights = jnp.clip(0.099609375 + 0.9003906 * jax.random.uniform(streams_of[2], (TOKENS, TOPK), jnp.float32) ** block_levels(streams_of[2], (TOKENS, TOPK), ((0, 16),), -0.2, 0.2), 0.099609375, 1.0).astype(jnp.bfloat16)
    cotangent = noise(streams_of[3], (TOKENS, D), 0.5, 3.0, ((0, 16),))
    w_gate = noise(streams_of[4], (EXPERTS, D, F), D ** -0.5, 0.125, ((0, 16), (2, 2)))
    w_up = noise(streams_of[5], (EXPERTS, D, F), D ** -0.5, 0.125, ((0, 16), (2, 2)))
    w_down = noise(streams_of[6], (EXPERTS, F, D), F ** -0.5, 0.25, ((0, 16), (1, 2)))
    return {"tokens": tokens, "expert_ids": expert_ids, "route_weights": route_weights, "cotangent": cotangent, "w_gate": w_gate, "w_up": w_up, "w_down": w_down}


def reference(tokens, expert_ids, route_weights, cotangent, w_gate, w_up, w_down):
    assigns = TOKENS * TOPK
    slot_total = N_EP * CAP
    quarter = F // N_TP
    flat_ids = expert_ids.reshape(-1).astype(jnp.int32)
    weight_flat = jnp.concatenate([route_weights.reshape(-1).astype(jnp.float32), jnp.zeros((1,), jnp.float32)])
    rows_pad = jnp.concatenate([tokens, jnp.zeros((1, D), jnp.bfloat16)], axis=0)
    cot_pad = jnp.concatenate([cotangent, jnp.zeros((1, D), jnp.bfloat16)], axis=0)

    def per_expert(expert):
        picked = jnp.nonzero(flat_ids == expert, size=slot_total, fill_value=assigns)[0].astype(jnp.int32)
        holder = (picked // TOPK).astype(jnp.int32)
        slot_rows = rows_pad[holder]
        slot_cot = cot_pad[holder]
        slot_scale = weight_flat[picked]
        gate_cols = w_gate[expert]
        up_cols = w_up[expert]
        down_rows_w = w_down[expert]
        gate_pre = jnp.dot(slot_rows, gate_cols, preferred_element_type=jnp.float32)
        up_pre = jnp.dot(slot_rows, up_cols, preferred_element_type=jnp.float32)
        hidden_back = lax.dot_general(slot_cot, down_rows_w, (((1,), (1,)), ((), ())), preferred_element_type=jnp.float32)
        gate_sig = jax.nn.sigmoid(gate_pre)
        activated = gate_pre * gate_sig
        hidden = activated * up_pre
        route_sum = jnp.sum(hidden * hidden_back, axis=1)
        hidden_cot = slot_scale[:, None] * hidden_back
        up_cot = (hidden_cot * activated).astype(jnp.bfloat16)
        gate_cot = (hidden_cot * up_pre * gate_sig * (1.0 + gate_pre * (1.0 - gate_sig))).astype(jnp.bfloat16)
        weighted_hidden = (slot_scale[:, None] * hidden).astype(jnp.bfloat16)
        grad_down_e = lax.dot_general(weighted_hidden, slot_cot, (((0,), (0,)), ((), ())), preferred_element_type=jnp.float32).astype(jnp.bfloat16)
        grad_gate_e = lax.dot_general(slot_rows, gate_cot, (((0,), (0,)), ((), ())), preferred_element_type=jnp.float32).astype(jnp.bfloat16)
        grad_up_e = lax.dot_general(slot_rows, up_cot, (((0,), (0,)), ((), ())), preferred_element_type=jnp.float32).astype(jnp.bfloat16)
        gate_blocks = gate_cot.astype(jnp.float32).reshape(slot_total, N_TP, quarter)
        up_blocks = up_cot.astype(jnp.float32).reshape(slot_total, N_TP, quarter)
        gate_w_blocks = gate_cols.astype(jnp.float32).reshape(D, N_TP, quarter)
        up_w_blocks = up_cols.astype(jnp.float32).reshape(D, N_TP, quarter)
        block_part = jnp.einsum('sjf,djf->sjd', gate_blocks, gate_w_blocks, precision=lax.Precision.HIGHEST)
        block_part = block_part + jnp.einsum('sjf,djf->sjd', up_blocks, up_w_blocks, precision=lax.Precision.HIGHEST)
        block_round = lax.optimization_barrier(block_part.astype(jnp.bfloat16))
        pair_grad = jnp.sum(block_round.astype(jnp.float32), axis=1).astype(jnp.bfloat16)
        return grad_gate_e, grad_up_e, grad_down_e, pair_grad, route_sum.astype(jnp.bfloat16), picked

    grad_gate, grad_up, grad_down, pair_grad, route_part, picked = lax.map(per_expert, jnp.arange(EXPERTS, dtype=jnp.int32))
    index_all = picked.reshape(-1)
    token_acc = jnp.zeros((assigns + 1, D), jnp.float32).at[index_all].set(pair_grad.reshape(-1, D).astype(jnp.float32))
    token_grad = jnp.sum(token_acc[:assigns].reshape(TOKENS, TOPK, D), axis=1).astype(jnp.bfloat16)
    route_acc = jnp.zeros((assigns + 1,), jnp.bfloat16).at[index_all].set(route_part.reshape(-1))
    route_grad = route_acc[:assigns].reshape(TOKENS, TOPK)
    gate_rows = jnp.sum(jnp.square(grad_gate.astype(jnp.float32)), axis=2)
    up_rows = jnp.sum(jnp.square(grad_up.astype(jnp.float32)), axis=2)
    down_rows = jnp.sum(jnp.square(grad_down.astype(jnp.float32)), axis=2)
    return (token_grad, route_grad, grad_gate, grad_up, grad_down, gate_rows, up_rows, down_rows)
```

```python
import functools

import jax
import jax.numpy as jnp
from jax import lax
from jax.experimental import pallas as pl
from jax.experimental.pallas import tpu as pltpu
from jax.sharding import PartitionSpec as P

MESH = pl.DeviceIdType.MESH
LANES = 128


def greet(experts, splits, me, col):
    barrier = pltpu.get_barrier_semaphore()

    @pl.loop(1, experts)
    def _(off):
        pl.semaphore_signal(
            barrier, inc=1, device_id={"ep": lax.rem(me + off, experts), "tp": col}, device_id_type=MESH
        )

    for shift in range(1, splits):
        pl.semaphore_signal(
            barrier, inc=1, device_id={"ep": me, "tp": lax.rem(col + shift, splits)}, device_id_type=MESH
        )
    pl.semaphore_wait(barrier, experts - 1 + splits - 1)


def remote(src, dst, send, recv, ep, tp):
    return pltpu.make_async_remote_copy(
        src_ref=src,
        dst_ref=dst,
        send_sem=send,
        recv_sem=recv,
        device_id={"ep": ep, "tp": tp},
        device_id_type=MESH,
    )


def dispatch_kernel(
    experts, splits, rows_ref, cot_ref, scale_ref, rows_out, cot_out, scale_out,
    send, recv, relay_send, relay_recv, local,
):
    me = lax.axis_index("ep")
    col = lax.axis_index("tp")
    width = rows_ref.shape[2]
    mine = pl.ds(pl.multiple_of(col * width, LANES), width)
    greet(experts, splits, me, col)
    pairs = ((rows_ref, rows_out), (cot_ref, cot_out))

    def out_copies(off):
        there = lax.rem(me + off, experts)
        copies = [
            remote(src.at[there], dst.at[me, :, mine], send.at[i, off], recv.at[i, off], there, col)
            for i, (src, dst) in enumerate(pairs)
        ]
        copies.append(
            remote(scale_ref.at[there], scale_out.at[me], send.at[2, off], recv.at[2, off], there, col)
        )
        return copies

    def relays(off, shift, i):
        source = lax.rem(me + experts - off, experts)
        block = pairs[i][1].at[source, :, mine]
        peer = lax.rem(col + shift, splits)
        return remote(block, block, relay_send.at[i, shift - 1, off], relay_recv.at[i, shift - 1, off], me, peer)

    own = [
        pltpu.make_async_copy(src.at[me], dst.at[me, :, mine], local.at[i])
        for i, (src, dst) in enumerate(pairs)
    ]
    own.append(pltpu.make_async_copy(scale_ref.at[me], scale_out.at[me], local.at[2]))
    for copy in own:
        copy.start()

    @pl.loop(1, experts)
    def _(off):
        for copy in out_copies(off):
            copy.start()

    for copy in own:
        copy.wait()
    for shift in range(1, splits):
        for i in range(2):
            relays(0, shift, i).start()

    @pl.loop(1, experts)
    def _(off):
        copies = out_copies(off)
        for i in range(2):
            copies[i].wait_recv()
            for shift in range(1, splits):
                relays(off, shift, i).start()

    @pl.loop(1, experts)
    def _(off):
        copies = out_copies(off)
        for copy in copies:
            copy.wait_send()
        copies[2].wait_recv()

    @pl.loop(0, experts)
    def _(off):
        for shift in range(1, splits):
            for i in range(2):
                relays(off, shift, i).wait_send()
                source = lax.rem(me + experts - off, experts)
                peer = lax.rem(col + splits - shift, splits)
                part = pl.ds(pl.multiple_of(peer * width, LANES), width)
                block = pairs[i][1].at[source, :, part]
                remote(
                    block, block, relay_send.at[i, shift - 1, off], relay_recv.at[i, shift - 1, off], me, peer
                ).wait_recv()


def dispatch(rows, cot, scale, experts, splits):
    capacity, width = rows.shape[1:]
    whole = jax.ShapeDtypeStruct((experts, capacity, width * splits), jnp.bfloat16)
    vmem = pl.BlockSpec(memory_space=pltpu.VMEM)
    return pl.pallas_call(
        functools.partial(dispatch_kernel, experts, splits),
        out_shape=(whole, whole, jax.ShapeDtypeStruct(scale.shape, scale.dtype)),
        in_specs=[vmem] * 3,
        out_specs=(vmem,) * 3,
        scratch_shapes=[
            pltpu.SemaphoreType.DMA((3, experts)),
            pltpu.SemaphoreType.DMA((3, experts)),
            pltpu.SemaphoreType.DMA((2, splits - 1, experts)),
            pltpu.SemaphoreType.DMA((2, splits - 1, experts)),
            pltpu.SemaphoreType.DMA((3,)),
        ],
        compiler_params=pltpu.CompilerParams(collective_id=0, has_side_effects=True),
    )(rows, cot, scale)


def combine_kernel(
    experts, splits, part_ref, route_ref, square_ref, back, back_route, square_out,
    peer_part, total, peer_route, route_total,
    swap_send, swap_recv, small_send, small_recv, send, recv,
):
    me = lax.axis_index("ep")
    col = lax.axis_index("tp")
    width = back.shape[2]
    mine = pl.ds(pl.multiple_of(col * width, LANES), width)
    greet(experts, splits, me, col)

    def swap(off, shift):
        source = lax.rem(me + off, experts)
        peer = lax.rem(col + shift, splits)
        theirs = pl.ds(pl.multiple_of(peer * width, LANES), width)
        return remote(
            part_ref.at[source, :, theirs], peer_part.at[shift - 1, source],
            swap_send.at[shift - 1, off], swap_recv.at[shift - 1, off], me, peer,
        )

    small = []
    for shift in range(1, splits):
        peer = lax.rem(col + shift, splits)
        small.append((
            remote(route_ref, peer_route.at[shift - 1], small_send.at[0, shift - 1],
                   small_recv.at[0, shift - 1], me, peer),
            remote(square_ref, square_out.at[shift - 1], small_send.at[1, shift - 1],
                   small_recv.at[1, shift - 1], me, peer),
        ))
    for shift in range(1, splits):
        small[shift - 1][0].start()

    @pl.loop(1, experts + 1)
    def _(step):
        for shift in range(1, splits):
            swap(lax.rem(step, experts), shift).start()

    for shift in range(1, splits):
        small[shift - 1][1].start()

    def block_total(off):
        source = lax.rem(me + off, experts)
        for shift in range(1, splits):
            swap(off, shift).wait_recv()
        value = part_ref[source, :, mine].astype(jnp.float32)
        for shift in range(1, splits):
            value = value + peer_part[shift - 1, source].astype(jnp.float32)
        return value.astype(back.dtype)

    def out_copies(off):
        there = lax.rem(me + off, experts)
        return (
            remote(total.at[there], back.at[me], send.at[0, off], recv.at[0, off], there, col),
            remote(route_total.at[there], back_route.at[me], send.at[1, off], recv.at[1, off], there, col),
        )

    value = route_ref[...]
    for shift in range(1, splits):
        small[shift - 1][0].wait_recv()
        value = value + peer_route[shift - 1]
    route_total[...] = value
    back_route[me] = route_total[me]

    @pl.loop(1, experts)
    def _(off):
        total[lax.rem(me + off, experts)] = block_total(off)
        for copy in out_copies(off):
            copy.start()

    back[me] = block_total(0)

    @pl.loop(1, experts)
    def _(off):
        for copy in out_copies(off):
            copy.wait()

    @pl.loop(0, experts)
    def _(off):
        for shift in range(1, splits):
            swap(off, shift).wait_send()

    for shift in range(1, splits):
        small[shift - 1][0].wait_send()
        small[shift - 1][1].wait()


def combine(part, route, squares, experts, splits):
    capacity, model_width = part.shape[1:]
    width = model_width // splits
    vmem = pl.BlockSpec(memory_space=pltpu.VMEM)
    return pl.pallas_call(
        functools.partial(combine_kernel, experts, splits),
        out_shape=(
            jax.ShapeDtypeStruct((experts, capacity, width), jnp.bfloat16),
            jax.ShapeDtypeStruct(route.shape, jnp.float32),
            jax.ShapeDtypeStruct((splits - 1,) + squares.shape, jnp.float32),
        ),
        in_specs=[vmem] * 3,
        out_specs=(vmem,) * 3,
        scratch_shapes=[
            pltpu.VMEM((splits - 1, experts, capacity, width), jnp.bfloat16),
            pltpu.VMEM((experts, capacity, width), jnp.bfloat16),
            pltpu.VMEM((splits - 1,) + route.shape, jnp.float32),
            pltpu.VMEM(route.shape, jnp.float32),
            pltpu.SemaphoreType.DMA((splits - 1, experts)),
            pltpu.SemaphoreType.DMA((splits - 1, experts)),
            pltpu.SemaphoreType.DMA((2, splits - 1)),
            pltpu.SemaphoreType.DMA((2, splits - 1)),
            pltpu.SemaphoreType.DMA((2, experts)),
            pltpu.SemaphoreType.DMA((2, experts)),
        ],
        compiler_params=pltpu.CompilerParams(collective_id=1, has_side_effects=True),
    )(part, route, squares)


def on_device(tokens, expert_ids, route_weights, cotangent, w_gate, w_up, w_down):
    tok_rows, model_width = tokens.shape
    topk = expert_ids.shape[1]
    experts = lax.axis_size("ep")
    splits = lax.axis_size("tp")
    capacity = 2 * tok_rows * topk // experts
    slot_count = experts * capacity
    f32, bf16 = jnp.float32, jnp.bfloat16

    expert_iota = jnp.arange(experts, dtype=jnp.int32)[None, :]
    slots = jnp.arange(slot_count, dtype=jnp.int32)[None, :]
    slot_expert = slots // capacity
    spread = (expert_iota.reshape(experts, 1) == slot_expert).astype(bf16)
    picks = [expert_ids[:, k : k + 1] == expert_iota for k in range(topk)]
    member = sum(p.astype(f32) for p in picks)
    weight = sum(
        jnp.where(p, route_weights[:, k : k + 1].astype(f32), 0.0) for k, p in enumerate(picks)
    ).astype(bf16)
    order = jnp.arange(tok_rows, dtype=jnp.int32)
    earlier = (order[:, None] > order[None, :]).astype(bf16)
    before = jnp.dot(earlier, member.astype(bf16), preferred_element_type=f32)
    rank = jnp.where(member > 0, before, -1.0).astype(bf16)
    slot_rank = jnp.dot(rank, spread, preferred_element_type=f32)
    chosen = slot_rank == (slots % capacity).astype(f32)
    select = chosen.astype(bf16)
    slot_weight = jnp.sum(
        jnp.where(chosen, jnp.dot(weight, spread, preferred_element_type=f32), 0.0), axis=0
    )
    width = model_width // splits
    start = lax.axis_index("tp") * width

    def pack(array):
        piece = lax.dynamic_slice_in_dim(array, start, width, 1)
        packed = lax.dot_general(select, piece, (((0,), (0,)), ((), ())), preferred_element_type=f32)
        return packed.astype(bf16).reshape(experts, capacity, width)

    lane_pad = -capacity % LANES
    scale_out = jnp.pad(slot_weight.reshape(experts, 1, capacity), ((0, 0), (0, 0), (0, lane_pad)))
    slot_rows, slot_cot, got_scale = dispatch(
        pack(tokens), pack(cotangent), scale_out, experts, splits
    )
    slot_rows = slot_rows.reshape(slot_count, model_width)
    slot_cot = slot_cot.reshape(slot_count, model_width)
    scale_col = got_scale[:, 0, :capacity].reshape(slot_count, 1)

    gate_cols = w_gate[0]
    up_cols = w_up[0]
    down_part = w_down[0]
    gate_pre = jnp.dot(slot_rows, gate_cols, preferred_element_type=f32)
    up_pre = jnp.dot(slot_rows, up_cols, preferred_element_type=f32)
    hidden_back = lax.dot_general(
        slot_cot, down_part, (((1,), (1,)), ((), ())), preferred_element_type=f32
    )
    gate_sig = jax.nn.sigmoid(gate_pre)
    activated = gate_pre * gate_sig
    hidden = activated * up_pre
    route_part = jnp.sum(hidden * hidden_back, axis=1)
    hidden_cot = scale_col * hidden_back
    up_cot = (hidden_cot * activated).astype(bf16)
    gate_cot = (hidden_cot * up_pre * gate_sig * (1.0 + gate_pre * (1.0 - gate_sig))).astype(bf16)
    weighted_hidden = (scale_col * hidden).astype(bf16)

    def outer(left, right):
        return lax.dot_general(
            left, right, (((0,), (0,)), ((), ())), preferred_element_type=f32
        ).astype(bf16)

    grad_down = outer(weighted_hidden, slot_cot)
    grad_gate = outer(slot_rows, gate_cot)
    grad_up = outer(slot_rows, up_cot)
    token_term = lax.dot_general(
        gate_cot, gate_cols, (((1,), (1,)), ((), ())), preferred_element_type=f32
    )
    token_term = token_term + lax.dot_general(
        up_cot, up_cols, (((1,), (1,)), ((), ())), preferred_element_type=f32
    )
    gate_square = jnp.sum(jnp.square(grad_gate.astype(f32)), axis=1)
    up_square = jnp.sum(jnp.square(grad_up.astype(f32)), axis=1)
    down_square = jnp.sum(jnp.square(grad_down.astype(f32)), axis=1)
    squares = jnp.stack([gate_square, up_square])
    route_out = jnp.pad(route_part.reshape(experts, 1, capacity), ((0, 0), (0, 0), (0, lane_pad)))
    back_rows, back_route, peer_squares = combine(
        token_term.astype(bf16).reshape(experts, capacity, model_width),
        route_out, squares, experts, splits,
    )
    squares = squares + jnp.sum(peer_squares, axis=0)
    token_grad = jnp.dot(
        select, back_rows.reshape(slot_count, width), preferred_element_type=f32
    ).astype(bf16)
    slot_route = back_route[:, 0, :capacity].reshape(1, slot_count)
    route_grad = jnp.concatenate(
        [
            jnp.sum(
                jnp.where(chosen & (slot_expert == expert_ids[:, k : k + 1]), slot_route, 0.0),
                axis=1, keepdims=True,
            )
            for k in range(topk)
        ],
        axis=1,
    ).astype(bf16)
    return (
        token_grad,
        route_grad,
        grad_gate[None],
        grad_up[None],
        grad_down[None],
        squares[0:1],
        squares[1:2],
        down_square[None],
    )


def solution(mesh):
    return jax.shard_map(
        on_device,
        mesh=mesh,
        in_specs=(
            P("ep", None),
            P("ep", None),
            P("ep", None),
            P("ep", None),
            P("ep", None, "tp"),
            P("ep", None, "tp"),
            P("ep", "tp", None),
        ),
        out_specs=(
            P("ep", "tp"),
            P("ep", None),
            P("ep", None, "tp"),
            P("ep", None, "tp"),
            P("ep", "tp", None),
            P("ep", None),
            P("ep", None),
            P("ep", "tp"),
        ),
        check_vma=False,
    )
```

```python
import functools

import jax
import jax.numpy as jnp
from jax import lax
from jax.experimental import pallas as pl
from jax.experimental.pallas import tpu as pltpu
from jax.sharding import PartitionSpec as P

MESH = pl.DeviceIdType.MESH
LANES = 128
SHARE = 4
GROUPS = 4


def greet(experts, splits, me, col):
    barrier = pltpu.get_barrier_semaphore()

    @pl.loop(1, experts)
    def _(off):
        pl.semaphore_signal(
            barrier, inc=1, device_id={"ep": lax.rem(me + off, experts), "tp": col}, device_id_type=MESH
        )

    for shift in range(1, splits):
        pl.semaphore_signal(
            barrier, inc=1, device_id={"ep": me, "tp": lax.rem(col + shift, splits)}, device_id_type=MESH
        )
    pl.semaphore_wait(barrier, experts - 1 + splits - 1)


def remote(src, dst, send, recv, ep, tp):
    return pltpu.make_async_remote_copy(
        src_ref=src,
        dst_ref=dst,
        send_sem=send,
        recv_sem=recv,
        device_id={"ep": ep, "tp": tp},
        device_id_type=MESH,
    )


def dispatch_kernel(
    experts, splits, rows_ref, cot_ref, choice_ref, scale_ref, rows_out, cot_out, scale_out,
    landed, landed_choice, stage, far_send, far_recv, send, recv, relay_send, relay_recv,
    scale_send, scale_recv, local,
):
    me = lax.axis_index("ep")
    col = lax.axis_index("tp")
    members = experts // GROUPS
    group = me // members
    seat = lax.rem(me, members)
    model_width = rows_out.shape[2]
    capacity = rows_out.shape[1]
    packed = rows_ref.shape[2]
    width = (model_width - packed) // (splits - 1) if splits > 1 else model_width
    shared = model_width - splits * width
    mine = pl.ds(pl.multiple_of(col * width, LANES), width)
    greet(experts, splits, me, col)
    inputs = (rows_ref, cot_ref, choice_ref)
    outputs = (rows_out, cot_out)
    views = [(i, pl.ds(0, width), mine) for i in range(2)]
    if shared:
        views += [(i, pl.ds(width, shared), pl.ds(splits * width, shared)) for i in range(2)]

    def far_copy(step, i):
        there = lax.rem(group + step, GROUPS)
        target = landed_choice.at[step] if i == 2 else landed.at[i, step]
        return remote(
            inputs[i].at[there], target, far_send.at[i, step], far_recv.at[i, step],
            there * members + seat, col,
        )

    def origin(step, hop):
        return lax.rem(group + GROUPS - step, GROUPS) * members + lax.rem(seat + members - hop, members)

    def near_copy(step, hop, n):
        i, here, there = views[n]
        target = lax.rem(seat + hop, members)
        return remote(
            stage.at[i, step, target, :, here], outputs[i].at[origin(step, 0), :, there],
            send.at[n, step, hop], recv.at[n, step, hop], group * members + target, col,
        )

    def own_copy(step, n):
        i, here, there = views[n]
        return pltpu.make_async_copy(
            stage.at[i, step, seat, :, here], outputs[i].at[origin(step, 0), :, there], local.at[n, step]
        )

    def relay(step, hop, shift, i, part):
        block = outputs[i].at[origin(step, hop), :, part]
        peer = lax.rem(col + shift, splits)
        return remote(
            block, block, relay_send.at[i, shift - 1, step, hop], relay_recv.at[i, shift - 1, step, hop], me, peer
        )

    def scale_copy(off):
        there = lax.rem(me + off, experts)
        return remote(
            scale_ref.at[there], scale_out.at[me], scale_send.at[off], scale_recv.at[off], there, col
        )

    scale_own = pltpu.make_async_copy(scale_ref.at[me], scale_out.at[me], local.at[4, 0])
    for step in range(1, GROUPS):
        for i in (2, 0, 1):
            far_copy(step, i).start()
    scale_own.start()

    for step in range(GROUPS):
        if step:
            far_copy(step, 2).wait_recv()
            choice = landed_choice[step]
        else:
            choice = choice_ref[group]
        for i in range(2):
            if step:
                far_copy(step, i).wait_recv()
                block = landed[i, step]
            else:
                block = inputs[i][group]
            spread = lax.dot_general(
                choice, block, (((0,), (0,)), ((), ())), preferred_element_type=jnp.float32
            )
            stage[i, step] = spread.astype(jnp.bfloat16).reshape(members, capacity, packed)
            for n in range(i, len(views), 2):
                own_copy(step, n).start()

            @pl.loop(1, members)
            def _(hop):
                near_copy(step, hop, i).start()

            if shared:

                @pl.loop(1, members)
                def _(hop):
                    near_copy(step, hop, i + 2).start()

        if step == 0:

            @pl.loop(1, experts)
            def _(off):
                scale_copy(off).start()

        for n in range(len(views)):
            own_copy(step, n).wait()
        for i in range(2):
            for shift in range(1, splits):
                relay(step, 0, shift, i, mine).start()

        @pl.loop(1, members)
        def _(hop):
            for i in range(2):
                near_copy(step, hop, i).wait_recv()
                for shift in range(1, splits):
                    relay(step, hop, shift, i, mine).start()

    scale_own.wait()

    @pl.loop(1, experts)
    def _(off):
        scale_copy(off).wait()

    for step in range(GROUPS):
        if step:
            for i in range(3):
                far_copy(step, i).wait_send()

        @pl.loop(1, members)
        def _(hop):
            for n in range(len(views)):
                near_copy(step, hop, n).wait_send()
                if n >= 2:
                    near_copy(step, hop, n).wait_recv()

        @pl.loop(0, members)
        def _(hop):
            for shift in range(1, splits):
                for i in range(2):
                    relay(step, hop, shift, i, mine).wait_send()
                    peer = lax.rem(col + splits - shift, splits)
                    part = pl.ds(pl.multiple_of(peer * width, LANES), width)
                    relay(step, hop, shift, i, part).wait_recv()


def dispatch(rows, cot, choice, scale, model_width, experts, splits):
    members = experts // GROUPS
    capacity = choice.shape[2] // members
    whole = jax.ShapeDtypeStruct((experts, capacity, model_width), jnp.bfloat16)
    vmem = pl.BlockSpec(memory_space=pltpu.VMEM)
    dma = pltpu.SemaphoreType.DMA
    return pl.pallas_call(
        functools.partial(dispatch_kernel, experts, splits),
        out_shape=(whole, whole, jax.ShapeDtypeStruct(scale.shape, scale.dtype)),
        in_specs=[vmem] * 4,
        out_specs=(vmem,) * 3,
        scratch_shapes=[
            pltpu.VMEM((2,) + rows.shape, jnp.bfloat16),
            pltpu.VMEM(choice.shape, jnp.bfloat16),
            pltpu.VMEM((2, GROUPS, members, capacity, rows.shape[2]), jnp.bfloat16),
            dma((3, GROUPS)),
            dma((3, GROUPS)),
            dma((4, GROUPS, members)),
            dma((4, GROUPS, members)),
            dma((2, splits - 1, GROUPS, members)),
            dma((2, splits - 1, GROUPS, members)),
            dma((experts,)),
            dma((experts,)),
            dma((5, GROUPS)),
        ],
        compiler_params=pltpu.CompilerParams(collective_id=0, has_side_effects=True),
    )(rows, cot, choice, scale)


def combine_kernel(
    experts, splits, part_ref, route_ref, square_ref, back, back_route, square_out,
    peer_part, total, peer_route, route_total,
    swap_send, swap_recv, small_send, small_recv, send, recv,
):
    me = lax.axis_index("ep")
    col = lax.axis_index("tp")
    width = back.shape[2]
    mine = pl.ds(pl.multiple_of(col * width, LANES), width)
    greet(experts, splits, me, col)

    def swap(off, shift):
        source = lax.rem(me + off, experts)
        peer = lax.rem(col + shift, splits)
        theirs = pl.ds(pl.multiple_of(peer * width, LANES), width)
        return remote(
            part_ref.at[source, :, theirs], peer_part.at[shift - 1, source],
            swap_send.at[shift - 1, off], swap_recv.at[shift - 1, off], me, peer,
        )

    small = []
    for shift in range(1, splits):
        peer = lax.rem(col + shift, splits)
        small.append((
            remote(route_ref, peer_route.at[shift - 1], small_send.at[0, shift - 1],
                   small_recv.at[0, shift - 1], me, peer),
            remote(square_ref, square_out.at[shift - 1], small_send.at[1, shift - 1],
                   small_recv.at[1, shift - 1], me, peer),
        ))
    for shift in range(1, splits):
        small[shift - 1][0].start()

    @pl.loop(1, experts + 1)
    def _(step):
        for shift in range(1, splits):
            swap(lax.rem(step, experts), shift).start()

    for shift in range(1, splits):
        small[shift - 1][1].start()

    def block_total(off):
        source = lax.rem(me + off, experts)
        for shift in range(1, splits):
            swap(off, shift).wait_recv()
        value = part_ref[source, :, mine].astype(jnp.float32)
        for shift in range(1, splits):
            value = value + peer_part[shift - 1, source].astype(jnp.float32)
        return value.astype(back.dtype)

    def out_copies(off):
        there = lax.rem(me + off, experts)
        return (
            remote(total.at[there], back.at[me], send.at[0, off], recv.at[0, off], there, col),
            remote(route_total.at[there], back_route.at[me], send.at[1, off], recv.at[1, off], there, col),
        )

    value = route_ref[...]
    for shift in range(1, splits):
        small[shift - 1][0].wait_recv()
        value = value + peer_route[shift - 1]
    route_total[...] = value
    back_route[me] = route_total[me]

    @pl.loop(1, experts)
    def _(off):
        total[lax.rem(me + off, experts)] = block_total(off)
        for copy in out_copies(off):
            copy.start()

    back[me] = block_total(0)

    @pl.loop(1, experts)
    def _(off):
        for copy in out_copies(off):
            copy.wait()

    @pl.loop(0, experts)
    def _(off):
        for shift in range(1, splits):
            swap(off, shift).wait_send()

    for shift in range(1, splits):
        small[shift - 1][0].wait_send()
        small[shift - 1][1].wait()


def combine(part, route, squares, experts, splits):
    capacity, model_width = part.shape[1:]
    width = model_width // splits
    vmem = pl.BlockSpec(memory_space=pltpu.VMEM)
    return pl.pallas_call(
        functools.partial(combine_kernel, experts, splits),
        out_shape=(
            jax.ShapeDtypeStruct((experts, capacity, width), jnp.bfloat16),
            jax.ShapeDtypeStruct(route.shape, jnp.float32),
            jax.ShapeDtypeStruct((splits - 1,) + squares.shape, jnp.float32),
        ),
        in_specs=[vmem] * 3,
        out_specs=(vmem,) * 3,
        scratch_shapes=[
            pltpu.VMEM((splits - 1, experts, capacity, width), jnp.bfloat16),
            pltpu.VMEM((experts, capacity, width), jnp.bfloat16),
            pltpu.VMEM((splits - 1,) + route.shape, jnp.float32),
            pltpu.VMEM(route.shape, jnp.float32),
            pltpu.SemaphoreType.DMA((splits - 1, experts)),
            pltpu.SemaphoreType.DMA((splits - 1, experts)),
            pltpu.SemaphoreType.DMA((2, splits - 1)),
            pltpu.SemaphoreType.DMA((2, splits - 1)),
            pltpu.SemaphoreType.DMA((2, experts)),
            pltpu.SemaphoreType.DMA((2, experts)),
        ],
        compiler_params=pltpu.CompilerParams(collective_id=1, has_side_effects=True),
    )(part, route, squares)


def on_device(tokens, expert_ids, route_weights, cotangent, w_gate, w_up, w_down):
    tok_rows, model_width = tokens.shape
    topk = expert_ids.shape[1]
    experts = lax.axis_size("ep")
    splits = lax.axis_size("tp")
    capacity = 2 * tok_rows * topk // experts
    slot_count = experts * capacity
    f32, bf16 = jnp.float32, jnp.bfloat16

    expert_iota = jnp.arange(experts, dtype=jnp.int32)[None, :]
    slots = jnp.arange(slot_count, dtype=jnp.int32)[None, :]
    slot_expert = slots // capacity
    spread = (expert_iota.reshape(experts, 1) == slot_expert).astype(bf16)
    picks = [expert_ids[:, k : k + 1] == expert_iota for k in range(topk)]
    member = sum(p.astype(f32) for p in picks)
    weight = sum(
        jnp.where(p, route_weights[:, k : k + 1].astype(f32), 0.0) for k, p in enumerate(picks)
    ).astype(bf16)
    order = jnp.arange(tok_rows, dtype=jnp.int32)
    earlier = (order[:, None] > order[None, :]).astype(bf16)
    before = jnp.dot(earlier, member.astype(bf16), preferred_element_type=f32)
    rank = jnp.where(member > 0, before, -1.0).astype(bf16)
    slot_rank = jnp.dot(rank, spread, preferred_element_type=f32)
    chosen = slot_rank == (slots % capacity).astype(f32)
    select = chosen.astype(bf16)
    slot_weight = jnp.sum(
        jnp.where(chosen, jnp.dot(weight, spread, preferred_element_type=f32), 0.0), axis=0
    )
    members = experts // GROUPS
    group_cap = members * capacity // topk
    group_slots = jnp.arange(GROUPS * group_cap, dtype=jnp.int32)[None, :]
    group_iota = jnp.arange(GROUPS, dtype=jnp.int32)[None, :]
    in_group = expert_ids[:, :1] // members == group_iota
    group_before = jnp.dot(earlier, in_group.astype(bf16), preferred_element_type=f32)
    own_rank = jnp.sum(jnp.where(in_group, group_before, 0.0), axis=1, keepdims=True).astype(jnp.int32)
    own_slot = expert_ids[:, :1] // members * group_cap + own_rank
    group_select = (own_slot == group_slots).astype(bf16)
    grouped = lax.dot_general(
        group_select, select, (((0,), (0,)), ((), ())), preferred_element_type=f32
    ).astype(bf16)
    span = members * capacity
    choice = jnp.stack(
        [
            grouped[g * group_cap : (g + 1) * group_cap, g * span : (g + 1) * span]
            for g in range(GROUPS)
        ]
    )
    width = model_width // splits
    shared = model_width // SHARE // (splits * LANES) * (splits * LANES) if SHARE else 0
    cut = (model_width - shared) // splits
    start = lax.axis_index("tp") * cut

    def pack(array):
        piece = jnp.concatenate(
            [lax.dynamic_slice_in_dim(array, start, cut, 1), array[:, splits * cut :]], axis=1
        )
        packed = lax.dot_general(
            group_select, piece, (((0,), (0,)), ((), ())), preferred_element_type=f32
        )
        return packed.astype(bf16).reshape(GROUPS, group_cap, cut + shared)

    lane_pad = -capacity % LANES
    scale_out = jnp.pad(slot_weight.reshape(experts, 1, capacity), ((0, 0), (0, 0), (0, lane_pad)))
    slot_rows, slot_cot, got_scale = dispatch(
        pack(tokens), pack(cotangent), choice, scale_out, model_width, experts, splits
    )
    slot_rows = slot_rows.reshape(slot_count, model_width)
    slot_cot = slot_cot.reshape(slot_count, model_width)
    scale_col = got_scale[:, 0, :capacity].reshape(slot_count, 1)

    gate_cols = w_gate[0]
    up_cols = w_up[0]
    down_part = w_down[0]
    gate_pre = jnp.dot(slot_rows, gate_cols, preferred_element_type=f32)
    up_pre = jnp.dot(slot_rows, up_cols, preferred_element_type=f32)
    hidden_back = lax.dot_general(
        slot_cot, down_part, (((1,), (1,)), ((), ())), preferred_element_type=f32
    )
    gate_sig = jax.nn.sigmoid(gate_pre)
    activated = gate_pre * gate_sig
    hidden = activated * up_pre
    route_part = jnp.sum(hidden * hidden_back, axis=1)
    hidden_cot = scale_col * hidden_back
    up_cot = (hidden_cot * activated).astype(bf16)
    gate_cot = (hidden_cot * up_pre * gate_sig * (1.0 + gate_pre * (1.0 - gate_sig))).astype(bf16)
    weighted_hidden = (scale_col * hidden).astype(bf16)

    def outer(left, right):
        return lax.dot_general(
            left, right, (((0,), (0,)), ((), ())), preferred_element_type=f32
        ).astype(bf16)

    grad_down = outer(weighted_hidden, slot_cot)
    grad_gate = outer(slot_rows, gate_cot)
    grad_up = outer(slot_rows, up_cot)
    token_term = lax.dot_general(
        gate_cot, gate_cols, (((1,), (1,)), ((), ())), preferred_element_type=f32
    )
    token_term = token_term + lax.dot_general(
        up_cot, up_cols, (((1,), (1,)), ((), ())), preferred_element_type=f32
    )
    gate_square = jnp.sum(jnp.square(grad_gate.astype(f32)), axis=1)
    up_square = jnp.sum(jnp.square(grad_up.astype(f32)), axis=1)
    down_square = jnp.sum(jnp.square(grad_down.astype(f32)), axis=1)
    squares = jnp.stack([gate_square, up_square])
    route_out = jnp.pad(route_part.reshape(experts, 1, capacity), ((0, 0), (0, 0), (0, lane_pad)))
    back_rows, back_route, peer_squares = combine(
        token_term.astype(bf16).reshape(experts, capacity, model_width),
        route_out, squares, experts, splits,
    )
    squares = squares + jnp.sum(peer_squares, axis=0)
    token_grad = jnp.dot(
        select, back_rows.reshape(slot_count, width), preferred_element_type=f32
    ).astype(bf16)
    slot_route = back_route[:, 0, :capacity].reshape(1, slot_count)
    route_grad = jnp.concatenate(
        [
            jnp.sum(
                jnp.where(chosen & (slot_expert == expert_ids[:, k : k + 1]), slot_route, 0.0),
                axis=1, keepdims=True,
            )
            for k in range(topk)
        ],
        axis=1,
    ).astype(bf16)
    return (
        token_grad,
        route_grad,
        grad_gate[None],
        grad_up[None],
        grad_down[None],
        squares[0:1],
        squares[1:2],
        down_square[None],
    )


def solution(mesh):
    return jax.shard_map(
        on_device,
        mesh=mesh,
        in_specs=(
            P("ep", None),
            P("ep", None),
            P("ep", None),
            P("ep", None),
            P("ep", None, "tp"),
            P("ep", None, "tp"),
            P("ep", "tp", None),
        ),
        out_specs=(
            P("ep", "tp"),
            P("ep", None),
            P("ep", None, "tp"),
            P("ep", None, "tp"),
            P("ep", "tp", None),
            P("ep", None),
            P("ep", None),
            P("ep", "tp"),
        ),
        check_vma=False,
    )
```

```python
import functools

import jax
import jax.numpy as jnp
from jax import lax
from jax.experimental import pallas as pl
from jax.experimental.pallas import tpu as pltpu
from jax.sharding import PartitionSpec as P

MESH = pl.DeviceIdType.MESH
LANES = 128
SHARE = 4
GROUPS = 4


def greet(experts, splits, me, col):
    barrier = pltpu.get_barrier_semaphore()

    @pl.loop(1, experts)
    def _(off):
        pl.semaphore_signal(
            barrier, inc=1, device_id={"ep": lax.rem(me + off, experts), "tp": col}, device_id_type=MESH
        )

    for shift in range(1, splits):
        pl.semaphore_signal(
            barrier, inc=1, device_id={"ep": me, "tp": lax.rem(col + shift, splits)}, device_id_type=MESH
        )
    pl.semaphore_wait(barrier, experts - 1 + splits - 1)


def remote(src, dst, send, recv, ep, tp):
    return pltpu.make_async_remote_copy(
        src_ref=src,
        dst_ref=dst,
        send_sem=send,
        recv_sem=recv,
        device_id={"ep": ep, "tp": tp},
        device_id_type=MESH,
    )


def dispatch_kernel(
    experts, splits, rows_ref, cot_ref, choice_ref, scale_ref, rows_out, cot_out, scale_out, landed_choice,
    landed, stage, far_send, far_recv, send, recv, relay_send, relay_recv,
    scale_send, scale_recv, local,
):
    me = lax.axis_index("ep")
    col = lax.axis_index("tp")
    members = experts // GROUPS
    group = me // members
    seat = lax.rem(me, members)
    model_width = rows_out.shape[2]
    capacity = rows_out.shape[1]
    packed = rows_ref.shape[2]
    width = (model_width - packed) // (splits - 1) if splits > 1 else model_width
    shared = model_width - splits * width
    mine = pl.ds(pl.multiple_of(col * width, LANES), width)
    greet(experts, splits, me, col)
    inputs = (rows_ref, cot_ref, choice_ref)
    outputs = (rows_out, cot_out)
    views = [(i, pl.ds(0, width), mine) for i in range(2)]
    if shared:
        views += [(i, pl.ds(width, shared), pl.ds(splits * width, shared)) for i in range(2)]

    def far_copy(step, i):
        there = lax.rem(group + step, GROUPS)
        target = landed_choice.at[step] if i == 2 else landed.at[i, step]
        return remote(
            inputs[i].at[there], target, far_send.at[i, step], far_recv.at[i, step],
            there * members + seat, col,
        )

    def origin(step, hop):
        return lax.rem(group + GROUPS - step, GROUPS) * members + lax.rem(seat + members - hop, members)

    def near_copy(step, hop, n):
        i, here, there = views[n]
        target = lax.rem(seat + hop, members)
        return remote(
            stage.at[i, step, target, :, here], outputs[i].at[origin(step, 0), :, there],
            send.at[n, step, hop], recv.at[n, step, hop], group * members + target, col,
        )

    def own_copy(step, n):
        i, here, there = views[n]
        return pltpu.make_async_copy(
            stage.at[i, step, seat, :, here], outputs[i].at[origin(step, 0), :, there], local.at[n, step]
        )

    def relay(step, hop, shift, i, part):
        block = outputs[i].at[origin(step, hop), :, part]
        peer = lax.rem(col + shift, splits)
        return remote(
            block, block, relay_send.at[i, shift - 1, step, hop], relay_recv.at[i, shift - 1, step, hop], me, peer
        )

    def scale_copy(off):
        there = lax.rem(me + off, experts)
        return remote(
            scale_ref.at[there], scale_out.at[me], scale_send.at[off], scale_recv.at[off], there, col
        )

    scale_own = pltpu.make_async_copy(scale_ref.at[me], scale_out.at[me], local.at[4, 0])
    for step in range(1, GROUPS):
        for i in (2, 0, 1):
            far_copy(step, i).start()
    scale_own.start()
    choice_own = pltpu.make_async_copy(choice_ref.at[group], landed_choice.at[0], local.at[4, 1])
    choice_own.start()

    for step in range(GROUPS):
        if step:
            far_copy(step, 2).wait_recv()
            choice = landed_choice[step]
        else:
            choice = choice_ref[group]
        for i in range(2):
            if step:
                far_copy(step, i).wait_recv()
                block = landed[i, step]
            else:
                block = inputs[i][group]
            spread = lax.dot_general(
                choice, block, (((0,), (0,)), ((), ())), preferred_element_type=jnp.float32
            )
            stage[i, step] = spread.astype(jnp.bfloat16).reshape(members, capacity, packed)
            for n in range(i, len(views), 2):
                own_copy(step, n).start()

            @pl.loop(1, members)
            def _(hop):
                near_copy(step, hop, i).start()

            if shared:

                @pl.loop(1, members)
                def _(hop):
                    near_copy(step, hop, i + 2).start()

        if step == 0:

            @pl.loop(1, experts)
            def _(off):
                scale_copy(off).start()

        for n in range(len(views)):
            own_copy(step, n).wait()
        for i in range(2):
            for shift in range(1, splits):
                relay(step, 0, shift, i, mine).start()

        @pl.loop(1, members)
        def _(hop):
            for i in range(2):
                near_copy(step, hop, i).wait_recv()
                for shift in range(1, splits):
                    relay(step, hop, shift, i, mine).start()

    scale_own.wait()
    choice_own.wait()

    @pl.loop(1, experts)
    def _(off):
        scale_copy(off).wait()

    for step in range(GROUPS):
        if step:
            for i in range(3):
                far_copy(step, i).wait_send()

        @pl.loop(1, members)
        def _(hop):
            for n in range(len(views)):
                near_copy(step, hop, n).wait_send()
                if n >= 2:
                    near_copy(step, hop, n).wait_recv()

        @pl.loop(0, members)
        def _(hop):
            for shift in range(1, splits):
                for i in range(2):
                    relay(step, hop, shift, i, mine).wait_send()
                    peer = lax.rem(col + splits - shift, splits)
                    part = pl.ds(pl.multiple_of(peer * width, LANES), width)
                    relay(step, hop, shift, i, part).wait_recv()


def dispatch(rows, cot, choice, scale, model_width, experts, splits):
    members = experts // GROUPS
    capacity = choice.shape[2] // members
    whole = jax.ShapeDtypeStruct((experts, capacity, model_width), jnp.bfloat16)
    vmem = pl.BlockSpec(memory_space=pltpu.VMEM)
    dma = pltpu.SemaphoreType.DMA
    return pl.pallas_call(
        functools.partial(dispatch_kernel, experts, splits),
        out_shape=(whole, whole, jax.ShapeDtypeStruct(scale.shape, scale.dtype),
                   jax.ShapeDtypeStruct(choice.shape, choice.dtype)),
        in_specs=[vmem] * 4,
        out_specs=(vmem,) * 4,
        scratch_shapes=[
            pltpu.VMEM((2,) + rows.shape, jnp.bfloat16),
            pltpu.VMEM((2, GROUPS, members, capacity, rows.shape[2]), jnp.bfloat16),
            dma((3, GROUPS)),
            dma((3, GROUPS)),
            dma((4, GROUPS, members)),
            dma((4, GROUPS, members)),
            dma((2, splits - 1, GROUPS, members)),
            dma((2, splits - 1, GROUPS, members)),
            dma((experts,)),
            dma((experts,)),
            dma((5, GROUPS)),
        ],
        compiler_params=pltpu.CompilerParams(collective_id=0, has_side_effects=True),
    )(rows, cot, choice, scale)


def combine_kernel(
    experts, splits, part_ref, route_ref, square_ref, choice_ref, back, back_route, square_out,
    peer_part, total, gathered, finished, peer_route, route_total,
    swap_send, swap_recv, small_send, small_recv, near_send, near_recv, far_send, far_recv,
    route_send, route_recv,
):
    me = lax.axis_index("ep")
    col = lax.axis_index("tp")
    members = experts // GROUPS
    group = me // members
    seat = lax.rem(me, members)
    capacity = part_ref.shape[1]
    width = back.shape[2]
    mine = pl.ds(pl.multiple_of(col * width, LANES), width)
    greet(experts, splits, me, col)
    order = tuple(range(1, GROUPS)) + (0,)

    def home(step, hop):
        return lax.rem(group + GROUPS - step, GROUPS) * members + lax.rem(seat + hop, members)

    def swap(step, hop, shift):
        source = home(step, hop)
        peer = lax.rem(col + shift, splits)
        theirs = pl.ds(pl.multiple_of(peer * width, LANES), width)
        return remote(
            part_ref.at[source, :, theirs], peer_part.at[shift - 1, source],
            swap_send.at[shift - 1, step, hop], swap_recv.at[shift - 1, step, hop], me, peer,
        )

    small = []
    for shift in range(1, splits):
        peer = lax.rem(col + shift, splits)
        small.append((
            remote(route_ref, peer_route.at[shift - 1], small_send.at[0, shift - 1],
                   small_recv.at[0, shift - 1], me, peer),
            remote(square_ref, square_out.at[shift - 1], small_send.at[1, shift - 1],
                   small_recv.at[1, shift - 1], me, peer),
        ))
    for shift in range(1, splits):
        small[shift - 1][0].start()

    for step in order:

        @pl.loop(1, members + 1)
        def _(turn):
            for shift in range(1, splits):
                swap(step, lax.rem(turn, members), shift).start()

    for shift in range(1, splits):
        small[shift - 1][1].start()

    def block_total(step, hop):
        source = home(step, hop)
        for shift in range(1, splits):
            swap(step, hop, shift).wait_recv()
        value = part_ref[source, :, mine].astype(jnp.float32)
        for shift in range(1, splits):
            value = value + peer_part[shift - 1, source].astype(jnp.float32)
        return value.astype(back.dtype)

    def near_copy(step, hop):
        target = lax.rem(seat + hop, members)
        return remote(
            total.at[step, hop], gathered.at[step, seat],
            near_send.at[step, hop], near_recv.at[step, hop], group * members + target, col,
        )

    def far_copy(step):
        return remote(
            finished.at[step], back.at[group], far_send.at[step], far_recv.at[step], home(step, 0), col
        )

    def route_copy(off):
        there = lax.rem(me + off, experts)
        return remote(
            route_total.at[there], back_route.at[me], route_send.at[off], route_recv.at[off], there, col
        )

    value = route_ref[...]
    for shift in range(1, splits):
        small[shift - 1][0].wait_recv()
        value = value + peer_route[shift - 1]
    route_total[...] = value
    back_route[me] = route_total[me]

    @pl.loop(1, experts)
    def _(off):
        route_copy(off).start()

    def spread(step):
        @pl.loop(1, members)
        def _(hop):
            total[step, hop] = block_total(step, hop)
            near_copy(step, hop).start()

        gathered[step, seat] = block_total(step, 0)

    def collect(step):
        @pl.loop(1, members)
        def _(hop):
            near_copy(step, hop).wait_recv()

        pairs = gathered[step].reshape(members * capacity, width)
        summed = jnp.dot(choice_ref[step], pairs, preferred_element_type=jnp.float32).astype(back.dtype)
        if step:
            finished[step] = summed
            far_copy(step).start()
        else:
            back[group] = summed

    for turn, step in enumerate(order):
        spread(step)
        if turn:
            collect(order[turn - 1])
    collect(order[-1])

    @pl.loop(1, experts)
    def _(off):
        route_copy(off).wait()

    for step in range(GROUPS):
        if step:
            far_copy(step).wait()

        @pl.loop(1, members)
        def _(hop):
            near_copy(step, hop).wait_send()

        @pl.loop(0, members)
        def _(hop):
            for shift in range(1, splits):
                swap(step, hop, shift).wait_send()

    for shift in range(1, splits):
        small[shift - 1][0].wait_send()
        small[shift - 1][1].wait()


def combine(part, route, squares, choice, experts, splits):
    capacity, model_width = part.shape[1:]
    width = model_width // splits
    members = experts // GROUPS
    group_cap = choice.shape[1]
    vmem = pl.BlockSpec(memory_space=pltpu.VMEM)
    dma = pltpu.SemaphoreType.DMA
    return pl.pallas_call(
        functools.partial(combine_kernel, experts, splits),
        out_shape=(
            jax.ShapeDtypeStruct((GROUPS, group_cap, width), jnp.bfloat16),
            jax.ShapeDtypeStruct(route.shape, jnp.float32),
            jax.ShapeDtypeStruct((splits - 1,) + squares.shape, jnp.float32),
        ),
        in_specs=[vmem] * 4,
        out_specs=(vmem,) * 3,
        scratch_shapes=[
            pltpu.VMEM((splits - 1, experts, capacity, width), jnp.bfloat16),
            pltpu.VMEM((GROUPS, members, capacity, width), jnp.bfloat16),
            pltpu.VMEM((GROUPS, members, capacity, width), jnp.bfloat16),
            pltpu.VMEM((GROUPS, group_cap, width), jnp.bfloat16),
            pltpu.VMEM((splits - 1,) + route.shape, jnp.float32),
            pltpu.VMEM(route.shape, jnp.float32),
            dma((splits - 1, GROUPS, members)),
            dma((splits - 1, GROUPS, members)),
            dma((2, splits - 1)),
            dma((2, splits - 1)),
            dma((GROUPS, members)),
            dma((GROUPS, members)),
            dma((GROUPS,)),
            dma((GROUPS,)),
            dma((experts,)),
            dma((experts,)),
        ],
        compiler_params=pltpu.CompilerParams(collective_id=1, has_side_effects=True),
    )(part, route, squares, choice)


def on_device(tokens, expert_ids, route_weights, cotangent, w_gate, w_up, w_down):
    tok_rows, model_width = tokens.shape
    topk = expert_ids.shape[1]
    experts = lax.axis_size("ep")
    splits = lax.axis_size("tp")
    capacity = 2 * tok_rows * topk // experts
    slot_count = experts * capacity
    f32, bf16 = jnp.float32, jnp.bfloat16

    expert_iota = jnp.arange(experts, dtype=jnp.int32)[None, :]
    slots = jnp.arange(slot_count, dtype=jnp.int32)[None, :]
    slot_expert = slots // capacity
    spread = (expert_iota.reshape(experts, 1) == slot_expert).astype(bf16)
    picks = [expert_ids[:, k : k + 1] == expert_iota for k in range(topk)]
    member = sum(p.astype(f32) for p in picks)
    weight = sum(
        jnp.where(p, route_weights[:, k : k + 1].astype(f32), 0.0) for k, p in enumerate(picks)
    ).astype(bf16)
    order = jnp.arange(tok_rows, dtype=jnp.int32)
    earlier = (order[:, None] > order[None, :]).astype(bf16)
    before = jnp.dot(earlier, member.astype(bf16), preferred_element_type=f32)
    rank = jnp.where(member > 0, before, -1.0).astype(bf16)
    slot_rank = jnp.dot(rank, spread, preferred_element_type=f32)
    chosen = slot_rank == (slots % capacity).astype(f32)
    select = chosen.astype(bf16)
    slot_weight = jnp.sum(
        jnp.where(chosen, jnp.dot(weight, spread, preferred_element_type=f32), 0.0), axis=0
    )
    members = experts // GROUPS
    group_cap = members * capacity // topk
    group_slots = jnp.arange(GROUPS * group_cap, dtype=jnp.int32)[None, :]
    group_iota = jnp.arange(GROUPS, dtype=jnp.int32)[None, :]
    in_group = expert_ids[:, :1] // members == group_iota
    group_before = jnp.dot(earlier, in_group.astype(bf16), preferred_element_type=f32)
    own_rank = jnp.sum(jnp.where(in_group, group_before, 0.0), axis=1, keepdims=True).astype(jnp.int32)
    own_slot = expert_ids[:, :1] // members * group_cap + own_rank
    group_select = (own_slot == group_slots).astype(bf16)
    grouped = lax.dot_general(
        group_select, select, (((0,), (0,)), ((), ())), preferred_element_type=f32
    ).astype(bf16)
    span = members * capacity
    choice = jnp.stack(
        [
            grouped[g * group_cap : (g + 1) * group_cap, g * span : (g + 1) * span]
            for g in range(GROUPS)
        ]
    )
    width = model_width // splits
    shared = model_width // SHARE // (splits * LANES) * (splits * LANES) if SHARE else 0
    cut = (model_width - shared) // splits
    start = lax.axis_index("tp") * cut

    def pack(array):
        piece = jnp.concatenate(
            [lax.dynamic_slice_in_dim(array, start, cut, 1), array[:, splits * cut :]], axis=1
        )
        packed = lax.dot_general(
            group_select, piece, (((0,), (0,)), ((), ())), preferred_element_type=f32
        )
        return packed.astype(bf16).reshape(GROUPS, group_cap, cut + shared)

    lane_pad = -capacity % LANES
    scale_out = jnp.pad(slot_weight.reshape(experts, 1, capacity), ((0, 0), (0, 0), (0, lane_pad)))
    slot_rows, slot_cot, got_scale, got_choice = dispatch(
        pack(tokens), pack(cotangent), choice, scale_out, model_width, experts, splits
    )
    slot_rows = slot_rows.reshape(slot_count, model_width)
    slot_cot = slot_cot.reshape(slot_count, model_width)
    scale_col = got_scale[:, 0, :capacity].reshape(slot_count, 1)

    gate_cols = w_gate[0]
    up_cols = w_up[0]
    down_part = w_down[0]
    gate_pre = jnp.dot(slot_rows, gate_cols, preferred_element_type=f32)
    up_pre = jnp.dot(slot_rows, up_cols, preferred_element_type=f32)
    hidden_back = lax.dot_general(
        slot_cot, down_part, (((1,), (1,)), ((), ())), preferred_element_type=f32
    )
    gate_sig = jax.nn.sigmoid(gate_pre)
    activated = gate_pre * gate_sig
    hidden = activated * up_pre
    route_part = jnp.sum(hidden * hidden_back, axis=1)
    hidden_cot = scale_col * hidden_back
    up_cot = (hidden_cot * activated).astype(bf16)
    gate_cot = (hidden_cot * up_pre * gate_sig * (1.0 + gate_pre * (1.0 - gate_sig))).astype(bf16)
    weighted_hidden = (scale_col * hidden).astype(bf16)

    def outer(left, right):
        return lax.dot_general(
            left, right, (((0,), (0,)), ((), ())), preferred_element_type=f32
        ).astype(bf16)

    grad_down = outer(weighted_hidden, slot_cot)
    grad_gate = outer(slot_rows, gate_cot)
    grad_up = outer(slot_rows, up_cot)
    token_term = lax.dot_general(
        gate_cot, gate_cols, (((1,), (1,)), ((), ())), preferred_element_type=f32
    )
    token_term = token_term + lax.dot_general(
        up_cot, up_cols, (((1,), (1,)), ((), ())), preferred_element_type=f32
    )
    gate_square = jnp.sum(jnp.square(grad_gate.astype(f32)), axis=1)
    up_square = jnp.sum(jnp.square(grad_up.astype(f32)), axis=1)
    down_square = jnp.sum(jnp.square(grad_down.astype(f32)), axis=1)
    squares = jnp.stack([gate_square, up_square])
    route_out = jnp.pad(route_part.reshape(experts, 1, capacity), ((0, 0), (0, 0), (0, lane_pad)))
    back_rows, back_route, peer_squares = combine(
        token_term.astype(bf16).reshape(experts, capacity, model_width),
        route_out, squares, got_choice, experts, splits,
    )
    squares = squares + jnp.sum(peer_squares, axis=0)
    token_grad = jnp.dot(
        group_select, back_rows.reshape(GROUPS * group_cap, width), preferred_element_type=f32
    ).astype(bf16)
    slot_route = back_route[:, 0, :capacity].reshape(1, slot_count)
    route_grad = jnp.concatenate(
        [
            jnp.sum(
                jnp.where(chosen & (slot_expert == expert_ids[:, k : k + 1]), slot_route, 0.0),
                axis=1, keepdims=True,
            )
            for k in range(topk)
        ],
        axis=1,
    ).astype(bf16)
    return (
        token_grad,
        route_grad,
        grad_gate[None],
        grad_up[None],
        grad_down[None],
        squares[0:1],
        squares[1:2],
        down_square[None],
    )


def solution(mesh):
    return jax.shard_map(
        on_device,
        mesh=mesh,
        in_specs=(
            P("ep", None),
            P("ep", None),
            P("ep", None),
            P("ep", None),
            P("ep", None, "tp"),
            P("ep", None, "tp"),
            P("ep", "tp", None),
        ),
        out_specs=(
            P("ep", "tp"),
            P("ep", None),
            P("ep", None, "tp"),
            P("ep", None, "tp"),
            P("ep", "tp", None),
            P("ep", None),
            P("ep", None),
            P("ep", "tp"),
        ),
        check_vma=False,
    )
```

```python
import functools

import jax
import jax.numpy as jnp
from jax import lax
from jax.experimental import pallas as pl
from jax.experimental.pallas import tpu as pltpu
from jax.sharding import PartitionSpec as P

MESH = pl.DeviceIdType.MESH
LANES = 128
SHARE = 3
GROUPS = 4


def greet(experts, splits, me, col):
    barrier = pltpu.get_barrier_semaphore()

    @pl.loop(1, experts)
    def _(off):
        pl.semaphore_signal(
            barrier, inc=1, device_id={"ep": lax.rem(me + off, experts), "tp": col}, device_id_type=MESH
        )

    for shift in range(1, splits):
        pl.semaphore_signal(
            barrier, inc=1, device_id={"ep": me, "tp": lax.rem(col + shift, splits)}, device_id_type=MESH
        )
    pl.semaphore_wait(barrier, experts - 1 + splits - 1)


def remote(src, dst, send, recv, ep, tp):
    return pltpu.make_async_remote_copy(
        src_ref=src,
        dst_ref=dst,
        send_sem=send,
        recv_sem=recv,
        device_id={"ep": ep, "tp": tp},
        device_id_type=MESH,
    )


def dispatch_kernel(
    experts, splits, rows_ref, cot_ref, choice_ref, scale_ref, rows_out, cot_out, scale_out, landed_choice,
    landed, stage, far_send, far_recv, send, recv, relay_send, relay_recv,
    scale_send, scale_recv, local,
):
    me = lax.axis_index("ep")
    col = lax.axis_index("tp")
    members = experts // GROUPS
    group = me // members
    seat = lax.rem(me, members)
    model_width = rows_out.shape[2]
    capacity = rows_out.shape[1]
    packed = rows_ref.shape[2]
    width = (model_width - packed) // (splits - 1) if splits > 1 else model_width
    shared = model_width - splits * width
    mine = pl.ds(pl.multiple_of(col * width, LANES), width)
    greet(experts, splits, me, col)
    inputs = (rows_ref, cot_ref, choice_ref)
    outputs = (rows_out, cot_out)
    views = [(i, pl.ds(0, width), mine) for i in range(2)]
    if shared:
        views += [(i, pl.ds(width, shared), pl.ds(splits * width, shared)) for i in range(2)]

    def far_copy(step, i):
        there = lax.rem(group + step, GROUPS)
        target = landed_choice.at[step] if i == 2 else landed.at[i, step]
        return remote(
            inputs[i].at[there], target, far_send.at[i, step], far_recv.at[i, step],
            there * members + seat, col,
        )

    def origin(step, hop):
        return lax.rem(group + GROUPS - step, GROUPS) * members + lax.rem(seat + members - hop, members)

    def near_copy(step, hop, n):
        i, here, there = views[n]
        target = lax.rem(seat + hop, members)
        return remote(
            stage.at[i, step, target, :, here], outputs[i].at[origin(step, 0), :, there],
            send.at[n, step, hop], recv.at[n, step, hop], group * members + target, col,
        )

    def own_copy(step, n):
        i, here, there = views[n]
        return pltpu.make_async_copy(
            stage.at[i, step, seat, :, here], outputs[i].at[origin(step, 0), :, there], local.at[n, step]
        )

    def relay(step, hop, shift, i, part):
        block = outputs[i].at[origin(step, hop), :, part]
        peer = lax.rem(col + shift, splits)
        return remote(
            block, block, relay_send.at[i, shift - 1, step, hop], relay_recv.at[i, shift - 1, step, hop], me, peer
        )

    def scale_copy(off):
        there = lax.rem(me + off, experts)
        return remote(
            scale_ref.at[there], scale_out.at[me], scale_send.at[off], scale_recv.at[off], there, col
        )

    scale_own = pltpu.make_async_copy(scale_ref.at[me], scale_out.at[me], local.at[4, 0])
    for step in range(1, GROUPS):
        for i in (2, 0, 1):
            far_copy(step, i).start()
    scale_own.start()
    choice_own = pltpu.make_async_copy(choice_ref.at[group], landed_choice.at[0], local.at[4, 1])
    choice_own.start()

    for step in range(GROUPS):
        if step:
            far_copy(step, 2).wait_recv()
            choice = landed_choice[step]
        else:
            choice = choice_ref[group]
        for i in range(2):
            if step:
                far_copy(step, i).wait_recv()
                block = landed[i, step]
            else:
                block = inputs[i][group]
            spread = lax.dot_general(
                choice, block, (((0,), (0,)), ((), ())), preferred_element_type=jnp.float32
            )
            stage[i, step] = spread.astype(jnp.bfloat16).reshape(members, capacity, packed)
            for n in range(i, len(views), 2):
                own_copy(step, n).start()

            @pl.loop(1, members)
            def _(hop):
                near_copy(step, hop, i).start()

        if shared:

            @pl.loop(1, members)
            def _(hop):
                for n in range(2, len(views)):
                    near_copy(step, hop, n).start()

        if step == 0:

            @pl.loop(1, experts)
            def _(off):
                scale_copy(off).start()

        for n in range(len(views)):
            own_copy(step, n).wait()
        for i in range(2):
            for shift in range(1, splits):
                relay(step, 0, shift, i, mine).start()

        @pl.loop(1, members)
        def _(hop):
            for i in range(2):
                near_copy(step, hop, i).wait_recv()
                for shift in range(1, splits):
                    relay(step, hop, shift, i, mine).start()

    scale_own.wait()
    choice_own.wait()

    @pl.loop(1, experts)
    def _(off):
        scale_copy(off).wait()

    for step in range(GROUPS):
        if step:
            for i in range(3):
                far_copy(step, i).wait_send()

        @pl.loop(1, members)
        def _(hop):
            for n in range(len(views)):
                near_copy(step, hop, n).wait_send()
                if n >= 2:
                    near_copy(step, hop, n).wait_recv()

        @pl.loop(0, members)
        def _(hop):
            for shift in range(1, splits):
                for i in range(2):
                    relay(step, hop, shift, i, mine).wait_send()
                    peer = lax.rem(col + splits - shift, splits)
                    part = pl.ds(pl.multiple_of(peer * width, LANES), width)
                    relay(step, hop, shift, i, part).wait_recv()


def dispatch(rows, cot, choice, scale, model_width, experts, splits):
    members = experts // GROUPS
    capacity = choice.shape[2] // members
    whole = jax.ShapeDtypeStruct((experts, capacity, model_width), jnp.bfloat16)
    vmem = pl.BlockSpec(memory_space=pltpu.VMEM)
    dma = pltpu.SemaphoreType.DMA
    return pl.pallas_call(
        functools.partial(dispatch_kernel, experts, splits),
        out_shape=(whole, whole, jax.ShapeDtypeStruct(scale.shape, scale.dtype),
                   jax.ShapeDtypeStruct(choice.shape, choice.dtype)),
        in_specs=[vmem] * 4,
        out_specs=(vmem,) * 4,
        scratch_shapes=[
            pltpu.VMEM((2,) + rows.shape, jnp.bfloat16),
            pltpu.VMEM((2, GROUPS, members, capacity, rows.shape[2]), jnp.bfloat16),
            dma((3, GROUPS)),
            dma((3, GROUPS)),
            dma((4, GROUPS, members)),
            dma((4, GROUPS, members)),
            dma((2, splits - 1, GROUPS, members)),
            dma((2, splits - 1, GROUPS, members)),
            dma((experts,)),
            dma((experts,)),
            dma((5, GROUPS)),
        ],
        compiler_params=pltpu.CompilerParams(collective_id=0, has_side_effects=True),
    )(rows, cot, choice, scale)


def combine_kernel(
    experts, splits, part_ref, route_ref, square_ref, choice_ref, back, back_route, square_out,
    peer_part, total, gathered, finished, peer_route, route_total,
    swap_send, swap_recv, small_send, small_recv, near_send, near_recv, far_send, far_recv,
    route_send, route_recv,
):
    me = lax.axis_index("ep")
    col = lax.axis_index("tp")
    members = experts // GROUPS
    group = me // members
    seat = lax.rem(me, members)
    capacity = part_ref.shape[1]
    width = back.shape[2]
    mine = pl.ds(pl.multiple_of(col * width, LANES), width)
    greet(experts, splits, me, col)
    order = tuple(range(1, GROUPS)) + (0,)

    def home(step, hop):
        return lax.rem(group + GROUPS - step, GROUPS) * members + lax.rem(seat + hop, members)

    def swap(step, hop, shift):
        source = home(step, hop)
        peer = lax.rem(col + shift, splits)
        theirs = pl.ds(pl.multiple_of(peer * width, LANES), width)
        return remote(
            part_ref.at[source, :, theirs], peer_part.at[shift - 1, source],
            swap_send.at[shift - 1, step, hop], swap_recv.at[shift - 1, step, hop], me, peer,
        )

    small = []
    for shift in range(1, splits):
        peer = lax.rem(col + shift, splits)
        small.append((
            remote(route_ref, peer_route.at[shift - 1], small_send.at[0, shift - 1],
                   small_recv.at[0, shift - 1], me, peer),
            remote(square_ref, square_out.at[shift - 1], small_send.at[1, shift - 1],
                   small_recv.at[1, shift - 1], me, peer),
        ))
    for shift in range(1, splits):
        small[shift - 1][0].start()

    for step in order:

        @pl.loop(1, members + 1)
        def _(turn):
            for shift in range(1, splits):
                swap(step, lax.rem(turn, members), shift).start()

    for shift in range(1, splits):
        small[shift - 1][1].start()

    def block_total(step, hop):
        source = home(step, hop)
        for shift in range(1, splits):
            swap(step, hop, shift).wait_recv()
        value = part_ref[source, :, mine].astype(jnp.float32)
        for shift in range(1, splits):
            value = value + peer_part[shift - 1, source].astype(jnp.float32)
        return value.astype(back.dtype)

    def near_copy(step, hop):
        target = lax.rem(seat + hop, members)
        return remote(
            total.at[step, hop], gathered.at[step, seat],
            near_send.at[step, hop], near_recv.at[step, hop], group * members + target, col,
        )

    def far_copy(step):
        return remote(
            finished.at[step], back.at[group], far_send.at[step], far_recv.at[step], home(step, 0), col
        )

    def route_copy(off):
        there = lax.rem(me + off, experts)
        return remote(
            route_total.at[there], back_route.at[me], route_send.at[off], route_recv.at[off], there, col
        )

    value = route_ref[...]
    for shift in range(1, splits):
        small[shift - 1][0].wait_recv()
        value = value + peer_route[shift - 1]
    route_total[...] = value
    back_route[me] = route_total[me]

    @pl.loop(1, experts)
    def _(off):
        route_copy(off).start()

    def spread(step):
        @pl.loop(1, members)
        def _(hop):
            total[step, hop] = block_total(step, hop)
            near_copy(step, hop).start()

        gathered[step, seat] = block_total(step, 0)

    def collect(step):
        @pl.loop(1, members)
        def _(hop):
            near_copy(step, hop).wait_recv()

        pairs = gathered[step].reshape(members * capacity, width)
        summed = jnp.dot(choice_ref[step], pairs, preferred_element_type=jnp.float32).astype(back.dtype)
        if step:
            finished[step] = summed
            far_copy(step).start()
        else:
            back[group] = summed

    for turn, step in enumerate(order):
        spread(step)
        if turn:
            collect(order[turn - 1])
    collect(order[-1])

    @pl.loop(1, experts)
    def _(off):
        route_copy(off).wait()

    for step in range(GROUPS):
        if step:
            far_copy(step).wait()

        @pl.loop(1, members)
        def _(hop):
            near_copy(step, hop).wait_send()

        @pl.loop(0, members)
        def _(hop):
            for shift in range(1, splits):
                swap(step, hop, shift).wait_send()

    for shift in range(1, splits):
        small[shift - 1][0].wait_send()
        small[shift - 1][1].wait()


def combine(part, route, squares, choice, experts, splits):
    capacity, model_width = part.shape[1:]
    width = model_width // splits
    members = experts // GROUPS
    group_cap = choice.shape[1]
    vmem = pl.BlockSpec(memory_space=pltpu.VMEM)
    dma = pltpu.SemaphoreType.DMA
    return pl.pallas_call(
        functools.partial(combine_kernel, experts, splits),
        out_shape=(
            jax.ShapeDtypeStruct((GROUPS, group_cap, width), jnp.bfloat16),
            jax.ShapeDtypeStruct(route.shape, jnp.float32),
            jax.ShapeDtypeStruct((splits - 1,) + squares.shape, jnp.float32),
        ),
        in_specs=[vmem] * 4,
        out_specs=(vmem,) * 3,
        scratch_shapes=[
            pltpu.VMEM((splits - 1, experts, capacity, width), jnp.bfloat16),
            pltpu.VMEM((GROUPS, members, capacity, width), jnp.bfloat16),
            pltpu.VMEM((GROUPS, members, capacity, width), jnp.bfloat16),
            pltpu.VMEM((GROUPS, group_cap, width), jnp.bfloat16),
            pltpu.VMEM((splits - 1,) + route.shape, jnp.float32),
            pltpu.VMEM(route.shape, jnp.float32),
            dma((splits - 1, GROUPS, members)),
            dma((splits - 1, GROUPS, members)),
            dma((2, splits - 1)),
            dma((2, splits - 1)),
            dma((GROUPS, members)),
            dma((GROUPS, members)),
            dma((GROUPS,)),
            dma((GROUPS,)),
            dma((experts,)),
            dma((experts,)),
        ],
        compiler_params=pltpu.CompilerParams(collective_id=1, has_side_effects=True),
    )(part, route, squares, choice)


def on_device(tokens, expert_ids, route_weights, cotangent, w_gate, w_up, w_down):
    tok_rows, model_width = tokens.shape
    topk = expert_ids.shape[1]
    experts = lax.axis_size("ep")
    splits = lax.axis_size("tp")
    capacity = 2 * tok_rows * topk // experts
    slot_count = experts * capacity
    f32, bf16 = jnp.float32, jnp.bfloat16

    expert_iota = jnp.arange(experts, dtype=jnp.int32)[None, :]
    slots = jnp.arange(slot_count, dtype=jnp.int32)[None, :]
    slot_expert = slots // capacity
    spread = (expert_iota.reshape(experts, 1) == slot_expert).astype(bf16)
    picks = [expert_ids[:, k : k + 1] == expert_iota for k in range(topk)]
    member = sum(p.astype(f32) for p in picks)
    weight = sum(
        jnp.where(p, route_weights[:, k : k + 1].astype(f32), 0.0) for k, p in enumerate(picks)
    ).astype(bf16)
    order = jnp.arange(tok_rows, dtype=jnp.int32)
    earlier = (order[:, None] > order[None, :]).astype(bf16)
    before = jnp.dot(earlier, member.astype(bf16), preferred_element_type=f32)
    rank = jnp.where(member > 0, before, -1.0).astype(bf16)
    slot_rank = jnp.dot(rank, spread, preferred_element_type=f32)
    chosen = slot_rank == (slots % capacity).astype(f32)
    select = chosen.astype(bf16)
    slot_weight = jnp.sum(
        jnp.where(chosen, jnp.dot(weight, spread, preferred_element_type=f32), 0.0), axis=0
    )
    members = experts // GROUPS
    group_cap = members * capacity // topk
    group_slots = jnp.arange(GROUPS * group_cap, dtype=jnp.int32)[None, :]
    group_iota = jnp.arange(GROUPS, dtype=jnp.int32)[None, :]
    in_group = expert_ids[:, :1] // members == group_iota
    group_before = jnp.dot(earlier, in_group.astype(bf16), preferred_element_type=f32)
    own_rank = jnp.sum(jnp.where(in_group, group_before, 0.0), axis=1, keepdims=True).astype(jnp.int32)
    own_slot = expert_ids[:, :1] // members * group_cap + own_rank
    group_select = (own_slot == group_slots).astype(bf16)
    grouped = lax.dot_general(
        group_select, select, (((0,), (0,)), ((), ())), preferred_element_type=f32
    ).astype(bf16)
    span = members * capacity
    choice = jnp.stack(
        [
            grouped[g * group_cap : (g + 1) * group_cap, g * span : (g + 1) * span]
            for g in range(GROUPS)
        ]
    )
    width = model_width // splits
    shared = model_width * SHARE // 8 // (splits * LANES) * (splits * LANES)
    cut = (model_width - shared) // splits
    start = lax.axis_index("tp") * cut

    def pack(array):
        piece = jnp.concatenate(
            [lax.dynamic_slice_in_dim(array, start, cut, 1), array[:, splits * cut :]], axis=1
        )
        packed = lax.dot_general(
            group_select, piece, (((0,), (0,)), ((), ())), preferred_element_type=f32
        )
        return packed.astype(bf16).reshape(GROUPS, group_cap, cut + shared)

    lane_pad = -capacity % LANES
    scale_out = jnp.pad(slot_weight.reshape(experts, 1, capacity), ((0, 0), (0, 0), (0, lane_pad)))
    slot_rows, slot_cot, got_scale, got_choice = dispatch(
        pack(tokens), pack(cotangent), choice, scale_out, model_width, experts, splits
    )
    slot_rows = slot_rows.reshape(slot_count, model_width)
    slot_cot = slot_cot.reshape(slot_count, model_width)
    scale_col = got_scale[:, 0, :capacity].reshape(slot_count, 1)

    gate_cols = w_gate[0]
    up_cols = w_up[0]
    down_part = w_down[0]
    gate_pre = jnp.dot(slot_rows, gate_cols, preferred_element_type=f32)
    up_pre = jnp.dot(slot_rows, up_cols, preferred_element_type=f32)
    hidden_back = lax.dot_general(
        slot_cot, down_part, (((1,), (1,)), ((), ())), preferred_element_type=f32
    )
    gate_sig = jax.nn.sigmoid(gate_pre)
    activated = gate_pre * gate_sig
    hidden = activated * up_pre
    route_part = jnp.sum(hidden * hidden_back, axis=1)
    hidden_cot = scale_col * hidden_back
    up_cot = (hidden_cot * activated).astype(bf16)
    gate_cot = (hidden_cot * up_pre * gate_sig * (1.0 + gate_pre * (1.0 - gate_sig))).astype(bf16)
    weighted_hidden = (scale_col * hidden).astype(bf16)

    def outer(left, right):
        return lax.dot_general(
            left, right, (((0,), (0,)), ((), ())), preferred_element_type=f32
        ).astype(bf16)

    grad_down = outer(weighted_hidden, slot_cot)
    grad_gate = outer(slot_rows, gate_cot)
    grad_up = outer(slot_rows, up_cot)
    token_term = lax.dot_general(
        gate_cot, gate_cols, (((1,), (1,)), ((), ())), preferred_element_type=f32
    )
    token_term = token_term + lax.dot_general(
        up_cot, up_cols, (((1,), (1,)), ((), ())), preferred_element_type=f32
    )
    gate_square = jnp.sum(jnp.square(grad_gate.astype(f32)), axis=1)
    up_square = jnp.sum(jnp.square(grad_up.astype(f32)), axis=1)
    down_square = jnp.sum(jnp.square(grad_down.astype(f32)), axis=1)
    squares = jnp.stack([gate_square, up_square])
    route_out = jnp.pad(route_part.reshape(experts, 1, capacity), ((0, 0), (0, 0), (0, lane_pad)))
    back_rows, back_route, peer_squares = combine(
        token_term.astype(bf16).reshape(experts, capacity, model_width),
        route_out, squares, got_choice, experts, splits,
    )
    squares = squares + jnp.sum(peer_squares, axis=0)
    token_grad = jnp.dot(
        group_select, back_rows.reshape(GROUPS * group_cap, width), preferred_element_type=f32
    ).astype(bf16)
    slot_route = back_route[:, 0, :capacity].reshape(1, slot_count)
    route_grad = jnp.concatenate(
        [
            jnp.sum(
                jnp.where(chosen & (slot_expert == expert_ids[:, k : k + 1]), slot_route, 0.0),
                axis=1, keepdims=True,
            )
            for k in range(topk)
        ],
        axis=1,
    ).astype(bf16)
    return (
        token_grad,
        route_grad,
        grad_gate[None],
        grad_up[None],
        grad_down[None],
        squares[0:1],
        squares[1:2],
        down_square[None],
    )


def solution(mesh):
    return jax.shard_map(
        on_device,
        mesh=mesh,
        in_specs=(
            P("ep", None),
            P("ep", None),
            P("ep", None),
            P("ep", None),
            P("ep", None, "tp"),
            P("ep", None, "tp"),
            P("ep", "tp", None),
        ),
        out_specs=(
            P("ep", "tp"),
            P("ep", None),
            P("ep", None, "tp"),
            P("ep", None, "tp"),
            P("ep", "tp", None),
            P("ep", None),
            P("ep", None),
            P("ep", "tp"),
        ),
        check_vma=False,
    )
```

```python
import functools

import jax
import jax.numpy as jnp
from jax import lax
from jax.experimental import pallas as pl
from jax.experimental.layout import Layout, with_layout_constraint
from jax.experimental.pallas import tpu as pltpu
from jax.sharding import PartitionSpec as P

MESH = pl.DeviceIdType.MESH
LANES = 128
SHARE = 4
GROUPS = 4


def greet(experts, splits, me, col):
    barrier = pltpu.get_barrier_semaphore()

    @pl.loop(1, experts)
    def _(off):
        pl.semaphore_signal(
            barrier, inc=1, device_id={"ep": lax.rem(me + off, experts), "tp": col}, device_id_type=MESH
        )

    for shift in range(1, splits):
        pl.semaphore_signal(
            barrier, inc=1, device_id={"ep": me, "tp": lax.rem(col + shift, splits)}, device_id_type=MESH
        )
    pl.semaphore_wait(barrier, experts - 1 + splits - 1)


def remote(src, dst, send, recv, ep, tp):
    return pltpu.make_async_remote_copy(
        src_ref=src,
        dst_ref=dst,
        send_sem=send,
        recv_sem=recv,
        device_id={"ep": ep, "tp": tp},
        device_id_type=MESH,
    )


def dispatch_kernel(
    experts, splits, rows_ref, cot_ref, choice_ref, scale_ref, rows_out, cot_out, scale_out, landed_choice,
    landed, stage, far_send, far_recv, send, recv, relay_send, relay_recv,
    scale_send, scale_recv, local,
):
    me = lax.axis_index("ep")
    col = lax.axis_index("tp")
    members = experts // GROUPS
    group = me // members
    seat = lax.rem(me, members)
    model_width = rows_out.shape[2]
    capacity = rows_out.shape[1]
    packed = rows_ref.shape[2]
    width = (model_width - packed) // (splits - 1) if splits > 1 else model_width
    shared = model_width - splits * width
    mine = pl.ds(pl.multiple_of(col * width, LANES), width)
    greet(experts, splits, me, col)
    inputs = (rows_ref, cot_ref, choice_ref)
    outputs = (rows_out, cot_out)
    views = [(i, pl.ds(0, width), mine) for i in range(2)]
    if shared:
        views += [(i, pl.ds(width, shared), pl.ds(splits * width, shared)) for i in range(2)]

    def far_copy(step, i):
        there = lax.rem(group + step, GROUPS)
        target = landed_choice.at[step] if i == 2 else landed.at[i, step]
        return remote(
            inputs[i].at[there], target, far_send.at[i, step], far_recv.at[i, step],
            there * members + seat, col,
        )

    def origin(step, hop):
        return lax.rem(group + GROUPS - step, GROUPS) * members + lax.rem(seat + members - hop, members)

    def near_copy(step, hop, n):
        i, here, there = views[n]
        target = lax.rem(seat + hop, members)
        return remote(
            stage.at[i, step, target, :, here], outputs[i].at[origin(step, 0), :, there],
            send.at[n, step, hop], recv.at[n, step, hop], group * members + target, col,
        )

    def own_copy(step, n):
        i, here, there = views[n]
        return pltpu.make_async_copy(
            stage.at[i, step, seat, :, here], outputs[i].at[origin(step, 0), :, there], local.at[n, step]
        )

    def relay(step, hop, shift, i, part):
        block = outputs[i].at[origin(step, hop), :, part]
        peer = lax.rem(col + shift, splits)
        return remote(
            block, block, relay_send.at[i, shift - 1, step, hop], relay_recv.at[i, shift - 1, step, hop], me, peer
        )

    def scale_copy(off):
        there = lax.rem(me + off, experts)
        return remote(
            scale_ref.at[there], scale_out.at[me], scale_send.at[off], scale_recv.at[off], there, col
        )

    scale_own = pltpu.make_async_copy(scale_ref.at[me], scale_out.at[me], local.at[4, 0])
    for step in range(1, GROUPS):
        for i in (2, 0, 1):
            far_copy(step, i).start()
    scale_own.start()
    choice_own = pltpu.make_async_copy(choice_ref.at[group], landed_choice.at[0], local.at[4, 1])
    choice_own.start()

    for step in range(GROUPS):
        if step:
            far_copy(step, 2).wait_recv()
            choice = landed_choice[step]
        else:
            choice = choice_ref[group]
        for i in range(2):
            if step:
                far_copy(step, i).wait_recv()
                block = landed[i, step]
            else:
                block = inputs[i][group]
            spread = lax.dot_general(
                choice, block, (((0,), (0,)), ((), ())), preferred_element_type=jnp.float32
            )
            stage[i, step] = spread.astype(jnp.bfloat16).reshape(members, capacity, packed)
            for n in range(i, len(views), 2):
                own_copy(step, n).start()

            @pl.loop(1, members)
            def _(hop):
                near_copy(step, hop, i).start()

            if shared:

                @pl.loop(1, members)
                def _(hop):
                    near_copy(step, hop, i + 2).start()

        if step == 0:

            @pl.loop(1, experts)
            def _(off):
                scale_copy(off).start()

        for n in range(len(views)):
            own_copy(step, n).wait()
        for i in range(2):
            for shift in range(1, splits):
                relay(step, 0, shift, i, mine).start()

        @pl.loop(1, members)
        def _(hop):
            for i in range(2):
                near_copy(step, hop, i).wait_recv()
                for shift in range(1, splits):
                    relay(step, hop, shift, i, mine).start()

    scale_own.wait()
    choice_own.wait()

    @pl.loop(1, experts)
    def _(off):
        scale_copy(off).wait()

    for step in range(GROUPS):
        if step:
            for i in range(3):
                far_copy(step, i).wait_send()

        @pl.loop(1, members)
        def _(hop):
            for n in range(len(views)):
                near_copy(step, hop, n).wait_send()
                if n >= 2:
                    near_copy(step, hop, n).wait_recv()

        @pl.loop(0, members)
        def _(hop):
            for shift in range(1, splits):
                for i in range(2):
                    relay(step, hop, shift, i, mine).wait_send()
                    peer = lax.rem(col + splits - shift, splits)
                    part = pl.ds(pl.multiple_of(peer * width, LANES), width)
                    relay(step, hop, shift, i, part).wait_recv()


def dispatch(rows, cot, choice, scale, model_width, experts, splits):
    members = experts // GROUPS
    capacity = choice.shape[2] // members
    whole = jax.ShapeDtypeStruct((experts, capacity, model_width), jnp.bfloat16)
    vmem = pl.BlockSpec(memory_space=pltpu.VMEM)
    dma = pltpu.SemaphoreType.DMA
    return pl.pallas_call(
        functools.partial(dispatch_kernel, experts, splits),
        out_shape=(whole, whole, jax.ShapeDtypeStruct(scale.shape, scale.dtype),
                   jax.ShapeDtypeStruct(choice.shape, choice.dtype)),
        in_specs=[vmem] * 4,
        out_specs=(vmem,) * 4,
        scratch_shapes=[
            pltpu.VMEM((2,) + rows.shape, jnp.bfloat16),
            pltpu.VMEM((2, GROUPS, members, capacity, rows.shape[2]), jnp.bfloat16),
            dma((3, GROUPS)),
            dma((3, GROUPS)),
            dma((4, GROUPS, members)),
            dma((4, GROUPS, members)),
            dma((2, splits - 1, GROUPS, members)),
            dma((2, splits - 1, GROUPS, members)),
            dma((experts,)),
            dma((experts,)),
            dma((5, GROUPS)),
        ],
        compiler_params=pltpu.CompilerParams(collective_id=0, has_side_effects=True),
    )(rows, cot, choice, scale)


def combine_kernel(
    experts, splits, part_ref, route_ref, square_ref, choice_ref, back, back_route, square_out,
    peer_part, total, gathered, finished, peer_route, route_total,
    swap_send, swap_recv, small_send, small_recv, near_send, near_recv, far_send, far_recv,
    route_send, route_recv,
):
    me = lax.axis_index("ep")
    col = lax.axis_index("tp")
    members = experts // GROUPS
    group = me // members
    seat = lax.rem(me, members)
    capacity = part_ref.shape[1]
    width = back.shape[2]
    mine = pl.ds(pl.multiple_of(col * width, LANES), width)
    greet(experts, splits, me, col)
    order = tuple(range(1, GROUPS)) + (0,)

    def home(step, hop):
        return lax.rem(group + GROUPS - step, GROUPS) * members + lax.rem(seat + hop, members)

    def swap(step, hop, shift):
        source = home(step, hop)
        peer = lax.rem(col + shift, splits)
        theirs = pl.ds(pl.multiple_of(peer * width, LANES), width)
        return remote(
            part_ref.at[source, :, theirs], peer_part.at[shift - 1, source],
            swap_send.at[shift - 1, step, hop], swap_recv.at[shift - 1, step, hop], me, peer,
        )

    small = []
    for shift in range(1, splits):
        peer = lax.rem(col + shift, splits)
        small.append((
            remote(route_ref, peer_route.at[shift - 1], small_send.at[0, shift - 1],
                   small_recv.at[0, shift - 1], me, peer),
            remote(square_ref, square_out.at[shift - 1], small_send.at[1, shift - 1],
                   small_recv.at[1, shift - 1], me, peer),
        ))
    for shift in range(1, splits):
        small[shift - 1][0].start()

    for step in order:

        @pl.loop(1, members + 1)
        def _(turn):
            for shift in range(1, splits):
                swap(step, lax.rem(turn, members), shift).start()

    for shift in range(1, splits):
        small[shift - 1][1].start()

    def block_total(step, hop):
        source = home(step, hop)
        for shift in range(1, splits):
            swap(step, hop, shift).wait_recv()
        value = part_ref[source, :, mine].astype(jnp.float32)
        for shift in range(1, splits):
            value = value + peer_part[shift - 1, source].astype(jnp.float32)
        return value.astype(back.dtype)

    def near_copy(step, hop):
        target = lax.rem(seat + hop, members)
        return remote(
            total.at[step, hop], gathered.at[step, seat],
            near_send.at[step, hop], near_recv.at[step, hop], group * members + target, col,
        )

    def far_copy(step):
        return remote(
            finished.at[step], back.at[group], far_send.at[step], far_recv.at[step], home(step, 0), col
        )

    def route_copy(off):
        there = lax.rem(me + off, experts)
        return remote(
            route_total.at[there], back_route.at[me], route_send.at[off], route_recv.at[off], there, col
        )

    value = route_ref[...]
    for shift in range(1, splits):
        small[shift - 1][0].wait_recv()
        value = value + peer_route[shift - 1]
    route_total[...] = value
    back_route[me] = route_total[me]

    @pl.loop(1, experts)
    def _(off):
        route_copy(off).start()

    def spread(step):
        @pl.loop(1, members)
        def _(hop):
            total[step, hop] = block_total(step, hop)
            near_copy(step, hop).start()

        gathered[step, seat] = block_total(step, 0)

    def collect(step):
        @pl.loop(1, members)
        def _(hop):
            near_copy(step, hop).wait_recv()

        pairs = gathered[step].reshape(members * capacity, width)
        summed = jnp.dot(choice_ref[step], pairs, preferred_element_type=jnp.float32).astype(back.dtype)
        if step:
            finished[step] = summed
            far_copy(step).start()
        else:
            back[group] = summed

    for turn, step in enumerate(order):
        spread(step)
        if turn:
            collect(order[turn - 1])
    collect(order[-1])

    @pl.loop(1, experts)
    def _(off):
        route_copy(off).wait()

    for step in range(GROUPS):
        if step:
            far_copy(step).wait()

        @pl.loop(1, members)
        def _(hop):
            near_copy(step, hop).wait_send()

        @pl.loop(0, members)
        def _(hop):
            for shift in range(1, splits):
                swap(step, hop, shift).wait_send()

    for shift in range(1, splits):
        small[shift - 1][0].wait_send()
        small[shift - 1][1].wait()


def combine(part, route, squares, choice, experts, splits):
    capacity, model_width = part.shape[1:]
    width = model_width // splits
    members = experts // GROUPS
    group_cap = choice.shape[1]
    vmem = pl.BlockSpec(memory_space=pltpu.VMEM)
    dma = pltpu.SemaphoreType.DMA
    return pl.pallas_call(
        functools.partial(combine_kernel, experts, splits),
        out_shape=(
            jax.ShapeDtypeStruct((GROUPS, group_cap, width), jnp.bfloat16),
            jax.ShapeDtypeStruct(route.shape, jnp.float32),
            jax.ShapeDtypeStruct((splits - 1,) + squares.shape, jnp.float32),
        ),
        in_specs=[vmem] * 4,
        out_specs=(vmem,) * 3,
        scratch_shapes=[
            pltpu.VMEM((splits - 1, experts, capacity, width), jnp.bfloat16),
            pltpu.VMEM((GROUPS, members, capacity, width), jnp.bfloat16),
            pltpu.VMEM((GROUPS, members, capacity, width), jnp.bfloat16),
            pltpu.VMEM((GROUPS, group_cap, width), jnp.bfloat16),
            pltpu.VMEM((splits - 1,) + route.shape, jnp.float32),
            pltpu.VMEM(route.shape, jnp.float32),
            dma((splits - 1, GROUPS, members)),
            dma((splits - 1, GROUPS, members)),
            dma((2, splits - 1)),
            dma((2, splits - 1)),
            dma((GROUPS, members)),
            dma((GROUPS, members)),
            dma((GROUPS,)),
            dma((GROUPS,)),
            dma((experts,)),
            dma((experts,)),
        ],
        compiler_params=pltpu.CompilerParams(collective_id=1, has_side_effects=True),
    )(part, route, squares, choice)


def on_device(tokens, expert_ids, route_weights, cotangent, w_gate, w_up, w_down):
    tok_rows, model_width = tokens.shape
    topk = expert_ids.shape[1]
    experts = lax.axis_size("ep")
    splits = lax.axis_size("tp")
    capacity = 2 * tok_rows * topk // experts
    slot_count = experts * capacity
    f32, bf16 = jnp.float32, jnp.bfloat16

    expert_iota = jnp.arange(experts, dtype=jnp.int32)[None, :]
    slots = jnp.arange(slot_count, dtype=jnp.int32)[None, :]
    slot_expert = slots // capacity
    spread = (expert_iota.reshape(experts, 1) == slot_expert).astype(bf16)
    picks = [expert_ids[:, k : k + 1] == expert_iota for k in range(topk)]
    member = sum(p.astype(f32) for p in picks)
    weight = sum(
        jnp.where(p, route_weights[:, k : k + 1].astype(f32), 0.0) for k, p in enumerate(picks)
    ).astype(bf16)
    order = jnp.arange(tok_rows, dtype=jnp.int32)
    earlier = (order[:, None] > order[None, :]).astype(bf16)
    before = jnp.dot(earlier, member.astype(bf16), preferred_element_type=f32)
    rank = jnp.where(member > 0, before, -1.0).astype(bf16)
    slot_rank = jnp.dot(rank, spread, preferred_element_type=f32)
    chosen = slot_rank == (slots % capacity).astype(f32)
    select = chosen.astype(bf16)
    slot_weight = jnp.sum(
        jnp.where(chosen, jnp.dot(weight, spread, preferred_element_type=f32), 0.0), axis=0
    )
    members = experts // GROUPS
    group_cap = members * capacity // topk
    group_slots = jnp.arange(GROUPS * group_cap, dtype=jnp.int32)[None, :]
    group_iota = jnp.arange(GROUPS, dtype=jnp.int32)[None, :]
    in_group = expert_ids[:, :1] // members == group_iota
    group_before = jnp.dot(earlier, in_group.astype(bf16), preferred_element_type=f32)
    own_rank = jnp.sum(jnp.where(in_group, group_before, 0.0), axis=1, keepdims=True).astype(jnp.int32)
    own_slot = expert_ids[:, :1] // members * group_cap + own_rank
    group_select = (own_slot == group_slots).astype(bf16)
    grouped = lax.dot_general(
        group_select, select, (((0,), (0,)), ((), ())), preferred_element_type=f32
    ).astype(bf16)
    span = members * capacity
    choice = jnp.stack(
        [
            grouped[g * group_cap : (g + 1) * group_cap, g * span : (g + 1) * span]
            for g in range(GROUPS)
        ]
    )
    width = model_width // splits
    shared = model_width // SHARE // (splits * LANES) * (splits * LANES) if SHARE else 0
    cut = (model_width - shared) // splits
    start = lax.axis_index("tp") * cut

    def pack(array):
        piece = jnp.concatenate(
            [lax.dynamic_slice_in_dim(array, start, cut, 1), array[:, splits * cut :]], axis=1
        )
        packed = lax.dot_general(
            group_select, piece, (((0,), (0,)), ((), ())), preferred_element_type=f32
        )
        return packed.astype(bf16).reshape(GROUPS, group_cap, cut + shared)

    lane_pad = -capacity % LANES
    scale_out = jnp.pad(slot_weight.reshape(experts, 1, capacity), ((0, 0), (0, 0), (0, lane_pad)))
    slot_rows, slot_cot, got_scale, got_choice = dispatch(
        pack(tokens), pack(cotangent), choice, scale_out, model_width, experts, splits
    )
    slot_rows = slot_rows.reshape(slot_count, model_width)
    slot_cot = slot_cot.reshape(slot_count, model_width)
    scale_col = got_scale[:, 0, :capacity].reshape(slot_count, 1)

    gate_cols = w_gate[0]
    up_cols = w_up[0]
    down_part = w_down[0]
    gate_pre = jnp.dot(slot_rows, gate_cols, preferred_element_type=f32)
    up_pre = jnp.dot(slot_rows, up_cols, preferred_element_type=f32)
    hidden_back = lax.dot_general(
        slot_cot, down_part, (((1,), (1,)), ((), ())), preferred_element_type=f32
    )
    gate_sig = jax.nn.sigmoid(gate_pre)
    activated = gate_pre * gate_sig
    hidden = activated * up_pre
    route_part = jnp.sum(hidden * hidden_back, axis=1)
    hidden_cot = scale_col * hidden_back
    up_cot = (hidden_cot * activated).astype(bf16)
    gate_cot = (hidden_cot * up_pre * gate_sig * (1.0 + gate_pre * (1.0 - gate_sig))).astype(bf16)
    weighted_hidden = (scale_col * hidden).astype(bf16)

    def outer(left, right):
        return lax.dot_general(
            left, right, (((0,), (0,)), ((), ())), preferred_element_type=f32
        ).astype(bf16)

    grad_down = outer(weighted_hidden, slot_cot)
    by_rows = Layout(major_to_minor=(0, 1))
    grad_gate = with_layout_constraint(outer(slot_rows, gate_cot), by_rows)
    grad_up = with_layout_constraint(outer(slot_rows, up_cot), by_rows)
    token_term = lax.dot_general(
        gate_cot, gate_cols, (((1,), (1,)), ((), ())), preferred_element_type=f32
    )
    token_term = token_term + lax.dot_general(
        up_cot, up_cols, (((1,), (1,)), ((), ())), preferred_element_type=f32
    )
    gate_square = jnp.sum(jnp.square(grad_gate.astype(f32)), axis=1)
    up_square = jnp.sum(jnp.square(grad_up.astype(f32)), axis=1)
    down_square = jnp.sum(jnp.square(grad_down.astype(f32)), axis=1)
    squares = jnp.stack([gate_square, up_square])
    route_out = jnp.pad(route_part.reshape(experts, 1, capacity), ((0, 0), (0, 0), (0, lane_pad)))
    back_rows, back_route, peer_squares = combine(
        token_term.astype(bf16).reshape(experts, capacity, model_width),
        route_out, squares, got_choice, experts, splits,
    )
    squares = squares + jnp.sum(peer_squares, axis=0)
    token_grad = jnp.dot(
        group_select, back_rows.reshape(GROUPS * group_cap, width), preferred_element_type=f32
    ).astype(bf16)
    slot_route = back_route[:, 0, :capacity].reshape(1, slot_count)
    route_grad = jnp.concatenate(
        [
            jnp.sum(
                jnp.where(chosen & (slot_expert == expert_ids[:, k : k + 1]), slot_route, 0.0),
                axis=1, keepdims=True,
            )
            for k in range(topk)
        ],
        axis=1,
    ).astype(bf16)
    return (
        token_grad,
        route_grad,
        grad_gate[None],
        grad_up[None],
        grad_down[None],
        squares[0:1],
        squares[1:2],
        down_square[None],
    )


def solution(mesh):
    return jax.shard_map(
        on_device,
        mesh=mesh,
        in_specs=(
            P("ep", None),
            P("ep", None),
            P("ep", None),
            P("ep", None),
            P("ep", None, "tp"),
            P("ep", None, "tp"),
            P("ep", "tp", None),
        ),
        out_specs=(
            P("ep", "tp"),
            P("ep", None),
            P("ep", None, "tp"),
            P("ep", None, "tp"),
            P("ep", "tp", None),
            P("ep", None),
            P("ep", None),
            P("ep", "tp"),
        ),
        check_vma=False,
    )
```
